32 devices in a mesh: rep: 4 (over z), fs: 4 (over y, x), tp: 2 (over core).
Axes of the slice: x: 2, y: 2, z: 4, core: 2. Of those that a mesh axis runs over, the one named last changes fastest.
Arguments:
- inputs: bfloat16 [2048, 2048], P('rep', 'fs'), may hold values from -6 to 6
- w_gate: bfloat16 [2048, 3072], P('fs', 'tp'), may hold values from -0.125 to 0.125
- w_up: bfloat16 [2048, 3072], P('fs', 'tp'), may hold values from -0.125 to 0.125
- conv_taps: bfloat16 [3, 3072], P(None, 'tp'), may hold values from -3.5 to 3.5
- w_down: bfloat16 [3072, 2048], P('tp', 'fs'), may hold values from -0.109375 to 0.109375
- out_grad: bfloat16 [2048, 2048], P('rep', 'fs'), may hold values from -6 to 6
Outputs:
- in_grad: bfloat16 [2048, 2048], P(('rep', 'tp'), 'fs')
- grad_gate: float32 [2048, 3072], P('fs', 'tp')
- grad_up: float32 [2048, 3072], P('fs', 'tp')
- grad_down: float32 [3072, 2048], P('tp', 'fs')
- grad_taps: float32 [3, 3072], P(None, 'tp')
- rows_gate: float32 [2048], P('fs')
- rows_up: float32 [2048], P('fs')
- rows_down: float32 [3072], P('tp')
The draws below stay inside these ranges and needn't reach their ends.
All inputs are finite; a program needn't handle non-finite values.
Results may differ from the reference program's by a relative error of at most 0.025.
Values may be sent and summed in bfloat16 or wider, within the bound.
A program may use at most 64 MiB of HBM per device.

```python
import jax
import jax.numpy as jnp
from jax import lax

D = 2048
FF = 3072
KW = 3
TOK = 512
TOKENS = 2048
N_REP = 4
N_FS = 4
N_TP = 2


def with_spikes(values, rng, source, target, shards_of, factor):
    owner, partner = [(jnp.arange(values.shape[dim]) // (values.shape[dim] // shards_of)).reshape([-1 if axis == dim else 1 for axis in range(values.ndim)]) for dim in (source, target)]
    chosen = jax.random.permutation(rng, shards_of)[partner]
    strong = (owner == chosen) | (owner == (partner + shards_of // 2) % shards_of)
    return jnp.where(strong, factor * values, values)


def levels(key, shape, split, low, high):
    def one(axis_at, blocks):
        draws = jax.random.uniform(jax.random.fold_in(jax.random.fold_in(key, 6), axis_at), (blocks,), jnp.float32, low / len(split), high / len(split))
        return jnp.repeat(jnp.exp(draws), shape[axis_at] // blocks).reshape((-1,) + (1,) * (len(shape) - axis_at - 1))

    level = one(*split[0])
    for cut in split[1:]:
        level = level * one(*cut)
    return level


def bell_draw(stream_key, extent, spread, most, pieces=(), kind=jnp.bfloat16):
    entries = jax.random.normal(stream_key, extent, jnp.float32) * spread
    if len(pieces) > 0:
        entries = levels(stream_key, extent, pieces, -0.22, 0.18) * entries
    return jnp.clip(entries, min=-most, max=most).astype(kind)


def noise_with(stream_key, shape, scale, reach, pieces, heavy, dtype=jnp.bfloat16):
    entries = scale * jax.random.normal(stream_key, shape, jnp.float32)
    if pieces:
        entries = entries * levels(stream_key, shape, pieces, -0.22, 0.18)
    return jnp.clip(with_spikes(entries, jax.random.fold_in(stream_key, 3), *heavy), -reach, reach).astype(dtype)


def setup_inputs(seed: int = 0) -> dict:
    streams_of = jax.random.split(jax.random.key(seed), 7)
    inputs = bell_draw(streams_of[0], (TOKENS, D), 1.0, 6.0, ((0, 4), (1, 4)))
    w_gate = bell_draw(streams_of[1], (D, FF), D ** -0.5, 0.125, ((0, 4), (1, 2)))
    w_up = bell_draw(streams_of[2], (D, FF), D ** -0.5, 0.125, ((0, 4), (1, 2)))
    conv_taps = bell_draw(streams_of[3], (KW, FF), KW ** -0.5, 3.5, ((1, 2),))
    w_down = bell_draw(streams_of[4], (FF, D), FF ** -0.5, 0.109375, ((0, 2), (1, 4)))
    out_grad = noise_with(streams_of[5], (TOKENS, D), 1.0, 6.0, ((0, 4), (1, 4)), (0, 1, 4, 2.0))
    return {"inputs": inputs, "w_gate": w_gate, "w_up": w_up, "conv_taps": conv_taps, "w_down": w_down, "out_grad": out_grad}


def rounded(values):
    return lax.optimization_barrier(values.astype(jnp.bfloat16)).astype(jnp.float32)


def shift_down(values, lag_rows):
    if lag_rows == 0:
        return values
    padding = jnp.zeros_like(values[:, :lag_rows])
    return jnp.concatenate([padding, values[:, :-lag_rows]], axis=1)


def shift_up(values, lag_rows):
    if lag_rows == 0:
        return values
    padding = jnp.zeros_like(values[:, :lag_rows])
    return jnp.concatenate([values[:, lag_rows:], padding], axis=1)


def contract(left, right, left_dim, right_dim):
    return lax.dot_general(left, right, (((left_dim,), (right_dim,)), ((), ())), preferred_element_type=jnp.float32)


def reference(inputs, w_gate, w_up, conv_taps, w_down, out_grad):
    block_width = D // N_FS
    hidden_block = FF // N_TP
    gate_sum = jnp.zeros((TOKENS, FF), jnp.float32)
    up_sum = jnp.zeros((TOKENS, FF), jnp.float32)
    act_sum = jnp.zeros((TOKENS, FF), jnp.float32)
    for block_id in range(N_FS):
        start_col = block_id * block_width
        end_col = start_col + block_width
        gate_sum = gate_sum + rounded(jnp.dot(inputs[:, start_col:end_col], w_gate[start_col:end_col], preferred_element_type=jnp.float32))
        up_sum = up_sum + rounded(jnp.dot(inputs[:, start_col:end_col], w_up[start_col:end_col], preferred_element_type=jnp.float32))
        act_sum = act_sum + rounded(contract(out_grad[:, start_col:end_col], w_down[:, start_col:end_col], 1, 1))
    gate_pre = gate_sum.astype(jnp.bfloat16)
    up_val = up_sum.astype(jnp.bfloat16)
    act_grad = act_sum.astype(jnp.bfloat16)
    tap_weights = conv_taps.astype(jnp.float32)
    gate_seq = gate_pre.astype(jnp.float32).reshape(N_REP, TOK, FF)
    up_seq = up_val.astype(jnp.float32).reshape(N_REP, TOK, FF)
    act_seq = act_grad.astype(jnp.float32).reshape(N_REP, TOK, FF)
    pre_act = jnp.zeros((N_REP, TOK, FF), jnp.float32)
    for tap_index in range(KW):
        pre_act = pre_act + tap_weights[tap_index] * shift_down(gate_seq, KW - 1 - tap_index)
    sigmoid_pre = jax.nn.sigmoid(pre_act)
    hidden = (pre_act * sigmoid_pre * up_seq).astype(jnp.bfloat16)
    up_grad = (act_seq * pre_act * sigmoid_pre).astype(jnp.bfloat16)
    pre_grad = act_seq * up_seq * sigmoid_pre * (1.0 + pre_act * (1.0 - sigmoid_pre))
    gate_grad = jnp.zeros((N_REP, TOK, FF), jnp.float32)
    tap_list = []
    for tap_index in range(KW):
        gate_grad = gate_grad + tap_weights[tap_index] * shift_up(pre_grad, KW - 1 - tap_index)
        tap_list.append(jnp.sum(shift_down(gate_seq, KW - 1 - tap_index) * pre_grad, axis=(0, 1)))
    grad_taps = jnp.stack(tap_list)
    gate_grad = gate_grad.astype(jnp.bfloat16).reshape(TOKENS, FF)
    up_grad = up_grad.reshape(TOKENS, FF)
    hidden = hidden.reshape(TOKENS, FF)
    input_sum = jnp.zeros((TOKENS, D), jnp.float32)
    for block_id in range(N_TP):
        start_col = block_id * hidden_block
        end_col = start_col + hidden_block
        term = contract(gate_grad[:, start_col:end_col], w_gate[:, start_col:end_col], 1, 1)
        term = term + contract(up_grad[:, start_col:end_col], w_up[:, start_col:end_col], 1, 1)
        input_sum = input_sum + rounded(term)
    in_grad = input_sum.astype(jnp.bfloat16)
    grad_gate = contract(inputs, gate_grad, 0, 0)
    grad_up = contract(inputs, up_grad, 0, 0)
    grad_down = contract(hidden, out_grad, 0, 0)
    rows_gate = jnp.sum(grad_gate * grad_gate, axis=1)
    rows_up = jnp.sum(grad_up * grad_up, axis=1)
    rows_down = jnp.sum(grad_down * grad_down, axis=1)
    return (in_grad, grad_gate, grad_up, grad_down, grad_taps, rows_gate, rows_up, rows_down)
```

```python
import functools

import jax
import jax.numpy as jnp
from jax import lax
from jax.experimental import pallas as pl
from jax.experimental.pallas import tpu as pltpu
from jax.sharding import PartitionSpec as P

KW = 3


def shift_down(values, lag_rows):
    if lag_rows == 0:
        return values
    padding = jnp.zeros_like(values[:lag_rows])
    return jnp.concatenate([padding, values[:-lag_rows]], axis=0)


def shift_up(values, lag_rows):
    if lag_rows == 0:
        return values
    padding = jnp.zeros_like(values[:lag_rows])
    return jnp.concatenate([values[lag_rows:], padding], axis=0)


def contract(left, right, left_dim, right_dim):
    return lax.dot_general(
        left, right, (((left_dim,), (right_dim,)), ((), ())), preferred_element_type=jnp.float32
    )


def row_norms(grad_gate, grad_up, grad_down):
    gate_rows = jnp.sum(grad_gate * grad_gate, axis=1)
    up_rows = jnp.sum(grad_up * grad_up, axis=1)
    down_rows = jnp.sum(grad_down * grad_down, axis=1)
    gate_rows, up_rows = lax.psum((gate_rows, up_rows), "tp")
    down_rows = lax.psum(down_rows, "fs")
    return (gate_rows, up_rows, down_rows)


def shards(inputs, w_gate, w_up, conv_taps, w_down, out_grad):
    tap_weights = conv_taps.astype(jnp.float32)
    gate_part = jnp.dot(inputs, w_gate, preferred_element_type=jnp.float32)
    up_part = jnp.dot(inputs, w_up, preferred_element_type=jnp.float32)
    act_part = contract(out_grad, w_down, 1, 1)
    gate_sum, up_sum, act_sum = (
        lax.psum(gate_part.astype(jnp.bfloat16), "fs").astype(jnp.float32),
        lax.psum(up_part.astype(jnp.bfloat16), "fs").astype(jnp.float32),
        lax.psum(act_part.astype(jnp.bfloat16), "fs").astype(jnp.float32),
    )
    gate_pre = gate_sum.astype(jnp.bfloat16)
    up_val = up_sum.astype(jnp.bfloat16)
    act_grad = act_sum.astype(jnp.bfloat16)
    gate_float = gate_pre.astype(jnp.float32)
    up_float = up_val.astype(jnp.float32)
    act_float = act_grad.astype(jnp.float32)
    shifted = [shift_down(gate_float, KW - 1 - tap_index) for tap_index in range(KW)]
    pre_act = tap_weights[0] * shifted[0]
    for tap_index in range(1, KW):
        pre_act = pre_act + tap_weights[tap_index] * shifted[tap_index]
    sigmoid_pre = jax.nn.sigmoid(pre_act)
    hidden = (pre_act * sigmoid_pre * up_float).astype(jnp.bfloat16)
    up_grad = (act_float * pre_act * sigmoid_pre).astype(jnp.bfloat16)
    pre_grad = act_float * up_float * sigmoid_pre * (1.0 + pre_act * (1.0 - sigmoid_pre))
    gate_acc = tap_weights[0] * shift_up(pre_grad, KW - 1)
    for tap_index in range(1, KW):
        gate_acc = gate_acc + tap_weights[tap_index] * shift_up(pre_grad, KW - 1 - tap_index)
    gate_grad = gate_acc.astype(jnp.bfloat16)
    gate_rows = gate_grad
    up_rows = up_grad
    in_grad = lax.psum_scatter(
        (contract(gate_rows, w_gate, 1, 1) + contract(up_rows, w_up, 1, 1)).astype(jnp.bfloat16),
        "tp",
        scatter_dimension=0,
        tiled=True,
    )
    grad_gate = contract(inputs, gate_grad, 0, 0)
    grad_up = contract(inputs, up_grad, 0, 0)
    grad_down = contract(hidden, out_grad, 0, 0)
    grad_taps = jnp.stack(
        [jnp.sum(shifted[tap_index] * pre_grad, axis=0) for tap_index in range(KW)]
    )
    grad_gate, grad_up, grad_down, grad_taps = (
        lax.psum(grad_gate.astype(jnp.bfloat16), "rep").astype(jnp.float32),
        lax.psum(grad_up.astype(jnp.bfloat16), "rep").astype(jnp.float32),
        lax.psum(grad_down.astype(jnp.bfloat16), "rep").astype(jnp.float32),
        lax.psum(grad_taps.astype(jnp.bfloat16), "rep").astype(jnp.float32),
    )
    gate_rows, up_rows, down_rows = row_norms(grad_gate, grad_up, grad_down)
    weight_grads = (grad_gate, grad_up, grad_down, grad_taps, gate_rows, up_rows, down_rows)
    grad_gate, grad_up, grad_down, grad_taps, gate_rows, up_rows, down_rows = weight_grads
    return (in_grad, grad_gate, grad_up, grad_down, grad_taps, gate_rows, up_rows, down_rows)


LANES = 128
CW = 256
HALO = 16
A_LAG = 2
B_LAG = 4
OUT_LAG = 10
RING = 4
MESH_ID = pl.DeviceIdType.MESH

STEPS = (
    (),
    (("forward", 0, 1), ("reduce", 1, 1)),
    (("forward", 0, 2),),
    (("reduce", 1, 2),),
    (("hidden", 1, 0),),
    (("grads", 1, 0), ("forward", 1, 0), ("gather", 1, 1), ("gather", 1, 2), ("reduce", 2, 0)),
)


def layer_kernel(
    n_rep, n_fs,
    x_hbm, wg_hbm, wu_hbm, taps_ref, wd_hbm, og_hbm,
    in_grad_ref, down_ref, gate_ref, up_ref, taps_out_ref, rows_gu_ref, rows_down_ref,
    x_ref, wg_ref, wu_ref, wd_ref, og_ref,
    xt, send_part, recv_part, held, h_all, g_all, u_all, ring, part, from_out, from_in, tot,
    acc, ig_send, ig_recv, tap_all, tap_two, tap_out, tap_in, tap_sum, rows_gu, rows_d, rows_tp, rows_fs,
    rs_send, rs_recv, ag_send, ag_recv, a_send, out_recv, in_recv, b_send, loc_sem, misc,
):
    tok, feat = x_ref.shape
    cw = CW
    chunks = wg_ref.shape[1] // cw
    subs = feat // cw
    own_rows = tok // 2
    span = own_rows + HALO
    slots = 3 * subs
    total_pieces = chunks * slots
    per = cw // LANES
    f32, bf16 = jnp.float32, jnp.bfloat16
    r = lax.axis_index("rep")
    f = lax.axis_index("fs")
    t = lax.axis_index("tp")
    half_rep = n_rep // 2
    is_left = r < half_rep
    toward = jnp.where(is_left, r + 1, r - 1)
    outward = jnp.where(is_left, r - 1, r + 1)
    is_end = jnp.logical_or(r == 0, r == n_rep - 1)
    is_mid = jnp.logical_not(is_end)
    beside = f + 1 - 2 * lax.rem(f, 2)
    across = lax.rem(f + 2, 4)
    corner = lax.rem(beside + 2, 4)
    peers = [beside, across, corner]
    side = lax.rem(f, 2)
    top = f // 2
    own_cols = pl.ds(pl.multiple_of(side * LANES, LANES), LANES)
    own_toks = pl.ds(pl.multiple_of(top * own_rows, own_rows), own_rows)

    barrier = pltpu.get_barrier_semaphore()
    for k in range(n_fs - 1):
        pl.semaphore_signal(barrier, inc=1, device_id={"fs": peers[k]}, device_id_type=MESH_ID)
    pl.semaphore_signal(barrier, inc=1, device_id={"tp": 1 - t}, device_id_type=MESH_ID)
    pl.semaphore_signal(barrier, inc=1, device_id={"rep": toward}, device_id_type=MESH_ID)

    @pl.when(is_mid)
    def _():
        pl.semaphore_signal(barrier, inc=1, device_id={"rep": outward}, device_id_type=MESH_ID)

    loads = []

    def load(src, dst):
        copy = pltpu.make_async_copy(src, dst, loc_sem.at[len(loads)])
        copy.start()
        loads.append(copy)

    first = slice(0, cw)
    load(x_hbm, x_ref)
    load(wg_hbm.at[:, first], wg_ref.at[:, first])
    load(wu_hbm.at[:, first], wu_ref.at[:, first])
    load(og_hbm, og_ref)
    load(wd_hbm.at[first], wd_ref.at[first])
    if chunks > 1:
        rest = slice(cw, chunks * cw)
        load(wg_hbm.at[:, rest], wg_ref.at[:, rest])
        load(wu_hbm.at[:, rest], wu_ref.at[:, rest])
        load(wd_hbm.at[rest], wd_ref.at[rest])

    def remote(src, dst, send, recv, device):
        return pltpu.make_async_remote_copy(
            src_ref=src, dst_ref=dst, send_sem=send, recv_sem=recv,
            device_id=device, device_id_type=MESH_ID,
        )

    def chunk_cols(c):
        if isinstance(c, int):
            return slice(c * cw, (c + 1) * cw)
        return pl.ds(pl.multiple_of(c * cw, cw), cw)

    def rs_copy(c, tensor, k):
        s = (c * 3 + tensor) * (n_fs - 1) + k
        return remote(
            send_part.at[c, tensor, peers[k]], recv_part.at[c, tensor, k],
            rs_send.at[s], rs_recv.at[s], {"fs": peers[k]},
        )

    def product(c, tensor):
        cols = chunk_cols(c)
        if tensor == 0:
            value = jnp.dot(x_ref[...], wg_ref[:, cols], preferred_element_type=f32)
        elif tensor == 1:
            value = jnp.dot(x_ref[...], wu_ref[:, cols], preferred_element_type=f32)
        else:
            value = contract(og_ref[...], wd_ref[cols, :], 1, 1)
        value = value.astype(bf16)
        for g in range(n_fs):
            row = (g // 2) * (own_rows - HALO)
            lane = (g % 2) * LANES
            send_part[c, tensor, g] = value[row : row + span, lane : lane + LANES]

    def reduce_send(c, tensor):
        for k in range(n_fs - 1):
            rs_copy(c, tensor, k).start()

    def reduce_start(c, tensor):
        product(c, tensor)
        reduce_send(c, tensor)

    def reduced(c, tensor):
        value = send_part[c, tensor, f].astype(f32)
        for k in range(n_fs - 1):
            rs_copy(c, tensor, k).wait_recv()
            value = value + recv_part[c, tensor, k].astype(f32)
        return value.astype(bf16).astype(f32)

    def block(c, tensor, owner, part_of=None):
        col = lax.rem(owner, 2) * LANES
        row = (owner // 2) * own_rows
        if tensor == 0:
            size = LANES if part_of is None else LANES // 2
            start = col + (0 if part_of is None else part_of * size)
            return h_all.at[
                c, pl.ds(pl.multiple_of(start, size), size), pl.ds(pl.multiple_of(row, own_rows), own_rows)
            ]
        size = own_rows if part_of is None else own_rows // 2
        start = row + (0 if part_of is None else part_of * size)
        ref = g_all if tensor == 1 else u_all
        return ref.at[c, pl.ds(pl.multiple_of(start, size), size), pl.ds(pl.multiple_of(col, LANES), LANES)]

    def ag_copy(c, tensor, step, owner):
        s = (c * 3 + tensor) * 4
        if step == 0:
            ref, slot, target = block(c, tensor, owner), 0, beside
        elif step == 1:
            ref, slot, target = block(c, tensor, owner), 1, across
        elif step == 2:
            ref, slot, target = block(c, tensor, owner, 1), 2, beside
        else:
            ref, slot, target = block(c, tensor, owner, 0), 3, across
        return remote(ref, ref, ag_send.at[s + slot], ag_recv.at[s + slot], {"fs": target})

    def gather_start(c, tensor):
        for step in (0, 1):
            ag_copy(c, tensor, step, f).start()

    def forward(c, tensor):
        ag_copy(c, tensor, 0, beside).wait_recv()
        ag_copy(c, tensor, 3, beside).start()
        ag_copy(c, tensor, 1, across).wait_recv()
        ag_copy(c, tensor, 2, across).start()

    def gathered(c, tensor):
        ag_copy(c, tensor, 2, corner).wait_recv()
        ag_copy(c, tensor, 3, corner).wait_recv()

    def own(value):
        return jnp.where(top == 0, value[:own_rows], value[HALO:])

    row_ids = lax.broadcasted_iota(jnp.int32, (span, LANES), 0)

    def down(value, lag):
        if lag == 0:
            return value
        return jnp.where(row_ids >= lag, pltpu.roll(value, lag, 0), 0.0)

    def up(value, lag):
        if lag == 0:
            return value
        return jnp.where(row_ids < span - lag, pltpu.roll(value, span - lag, 0), 0.0)

    def own_weights(c):
        cols = pl.ds(pl.multiple_of(c * cw + side * LANES, LANES), LANES)
        return taps_ref[:, cols].astype(f32)

    def hidden_step(c):
        weights = own_weights(c)
        gate = reduced(c, 0)
        pre = weights[0:1] * down(gate, KW - 1)
        for j in range(1, KW):
            pre = pre + weights[j : j + 1] * down(gate, KW - 1 - j)
        sig = 1.0 / (1.0 + jnp.exp(-pre))
        up_val = reduced(c, 1)
        h_all[c, own_cols, own_toks] = own(pre * sig * up_val).T.astype(bf16)
        gather_start(c, 0)
        held[0] = gate
        held[1] = up_val
        held[2] = pre
        held[3] = sig

    def grads_step(c):
        weights = own_weights(c)
        gate, up_val, pre, sig = held[0], held[1], held[2], held[3]
        act = reduced(c, 2)
        pre_grad = act * up_val * sig * (1.0 + pre * (1.0 - sig))
        grad = weights[0:1] * up(pre_grad, KW - 1)
        for j in range(1, KW):
            grad = grad + weights[j : j + 1] * up(pre_grad, KW - 1 - j)
        g_all[c, own_toks, own_cols] = own(grad).astype(bf16)
        u_all[c, own_toks, own_cols] = own(act * (pre * sig)).astype(bf16)
        for j in range(KW):
            tap_all[f, pl.ds(c * KW + j, 1), :] = jnp.sum(
                own(down(gate, KW - 1 - j) * pre_grad), axis=0, keepdims=True
            )

    def part_copy(p):
        return remote(part.at[p], from_out.at[p], a_send.at[p], out_recv.at[p], {"rep": toward})

    def exchange_copy(p):
        return remote(part.at[p], from_in.at[p], a_send.at[p], in_recv.at[p], {"rep": toward})

    def total_copy(p, src):
        return remote(src.at[p], from_in.at[p], b_send.at[p], in_recv.at[p], {"rep": outward})

    def finished(c, s, value):
        tensor, q = s // subs, s % subs
        inner = slice(q * cw, (q + 1) * cw)
        if tensor == 0:
            down_ref[chunk_cols(c), inner] = value
        elif tensor == 1:
            gate_ref[inner, chunk_cols(c)] = value
        else:
            up_ref[inner, chunk_cols(c)] = value
        value = value.astype(f32)
        square = value * value
        lanes = square[:, :LANES]
        for g in range(1, cw // LANES):
            lanes = lanes + square[:, g * LANES : (g + 1) * LANES]
        for i in range(per):
            row = jnp.sum(lanes[i * LANES : (i + 1) * LANES].T, axis=0, keepdims=True)
            if tensor == 0:
                at = pl.ds(c * per + i, 1)
                rows_d[at, :] = row if q == 0 else rows_d[at, :] + row
            else:
                at = ((tensor - 1) * subs + q) * per + i
                rows_gu[at : at + 1, :] = rows_gu[at : at + 1, :] + row

    def stage_a(p):
        part_copy(p).wait_recv()
        part[p] = (ring[lax.rem(p, RING)] + from_out[p].astype(f32)).astype(bf16)
        exchange_copy(p).start()

    def stage_b(c, s):
        p = c * slots + s
        exchange_copy(p).wait_recv()
        value = (part[p].astype(f32) + from_in[p].astype(f32)).astype(bf16)
        tot[p] = value
        total_copy(p, tot).start()
        finished(c, s, value)

    def stage_out(c, s):
        exchange_copy(c * slots + s).wait_recv()
        finished(c, s, from_in[c * slots + s])

    def behind(c, s, lag):
        back = (lag - s + slots - 1) // slots if lag > s else 0
        return c - back, s - lag + back * slots, back

    def guarded(c, lowest, fn):
        if isinstance(c, int):
            if c >= lowest:
                fn()
        elif lowest <= 1:
            fn()
        else:
            pl.when(c >= lowest)(fn)

    def work(c, s):
        tensor, q = s // subs, s % subs
        p = c * slots + s
        if q == 0:
            gathered(c, tensor)
        if tensor == 0:
            value = jnp.dot(h_all[c], og_ref[:, q * cw : (q + 1) * cw], preferred_element_type=f32)
        elif tensor == 1:
            value = jnp.dot(xt[q], g_all[c], preferred_element_type=f32)
        else:
            value = jnp.dot(xt[q], u_all[c], preferred_element_type=f32)
        ca, sa, ka = behind(c, s, A_LAG)
        cb, sb, kb = behind(c, s, B_LAG)
        co, so, ko = behind(c, s, OUT_LAG)

        @pl.when(is_end)
        def _():
            part[p] = value.astype(bf16)
            part_copy(p).start()
            guarded(c, ko, lambda: stage_out(co, so))

        @pl.when(is_mid)
        def _():
            ring[lax.rem(p, RING)] = value
            guarded(c, ka, lambda: stage_a(ca * slots + sa))
            guarded(c, kb, lambda: stage_b(cb, sb))

    def input_term(c):
        cols = chunk_cols(c)
        term = contract(g_all[c], wg_ref[:, cols], 1, 1) + contract(u_all[c], wu_ref[:, cols], 1, 1)
        if isinstance(c, int) and c == 0:
            acc[...] = term
        else:
            acc[...] += term

    actions = {
        "forward": forward,
        "reduce": reduce_start,
        "hidden": lambda c, tensor: hidden_step(c),
        "grads": lambda c, tensor: grads_step(c),
        "gather": gather_start,
    }

    def run(step, c):
        name, ahead, tensor = step
        target = c + ahead
        if isinstance(c, int):
            if target < chunks:
                actions[name](target, tensor)
        elif ahead == 0:
            actions[name](target, tensor)
        else:
            pl.when(target < chunks)(lambda: actions[name](target, tensor))

    def body(c):
        for s in range(slots):
            for step in STEPS[s]:
                run(step, c)
            work(c, s)
        input_term(c)

    loads[0].wait()
    loads[1].wait()
    product(0, 0)
    loads[2].wait()
    product(0, 1)
    pl.semaphore_wait(barrier, n_fs + 1 + jnp.where(is_mid, 1, 0))
    reduce_send(0, 0)
    reduce_send(0, 1)
    loads[3].wait()
    loads[4].wait()
    reduce_start(0, 2)
    for q in range(subs):
        xt[q] = x_ref[:, q * cw : (q + 1) * cw].astype(f32).T.astype(bf16)
    rows_gu[...] = jnp.zeros_like(rows_gu)
    for copy in loads[5:]:
        copy.wait()
    hidden_step(0)
    grads_step(0)
    forward(0, 0)
    gather_start(0, 1)
    gather_start(0, 2)
    if chunks > 1:
        reduce_start(1, 0)
    body(0)

    @pl.loop(1, chunks)
    def _(c):
        body(c)

    m = 2 * (n_fs - 1)
    half = tok // 2
    ig_send[...] = acc[...].astype(bf16)
    ig_copy = remote(
        ig_send.at[pl.ds(pl.multiple_of((1 - t) * half, half), half)], ig_recv,
        misc.at[m], misc.at[m + 1], {"tp": 1 - t},
    )
    ig_copy.start()

    tap_peers = []
    for k in range(n_fs - 1):
        tap_peers.append(remote(
            tap_all.at[f], tap_all.at[f], misc.at[2 * k], misc.at[2 * k + 1], {"fs": peers[k]}
        ))
        tap_peers[k].start()
    tap_part = remote(tap_two, tap_out, misc.at[m + 2], misc.at[m + 3], {"rep": toward})
    tap_exchange = remote(tap_two, tap_in, misc.at[m + 2], misc.at[m + 4], {"rep": toward})
    tap_total = remote(tap_sum, tap_in, misc.at[m + 5], misc.at[m + 4], {"rep": outward})

    def tap_first():
        for copy in tap_peers:
            copy.wait()
        for i in range(per):
            tap_two[i] = tap_all[i] + tap_all[i + 2]

    def input_finish():
        ig_copy.wait()
        in_grad_ref[...] = (
            ig_send[pl.ds(pl.multiple_of(t * half, half), half), :].astype(f32) + ig_recv[...].astype(f32)
        ).astype(bf16)

    fs_rows = [
        remote(rows_d, rows_fs.at[k], misc.at[m + 8 + 2 * k], misc.at[m + 9 + 2 * k], {"fs": peers[k]})
        for k in range(n_fs - 1)
    ]
    tp_rows = remote(rows_gu, rows_tp, misc.at[m + 6], misc.at[m + 7], {"tp": 1 - t})

    def rows_done(p, lag):
        if p == total_pieces - min(lag, slots - subs + 1):
            for copy in fs_rows:
                copy.start()
        if p == total_pieces - 1:
            tp_rows.start()

    @pl.when(is_end)
    def _():
        tap_first()
        tap_part.start()
        input_finish()
        for p in range(total_pieces - OUT_LAG, total_pieces):
            stage_out(p // slots, p % slots)
            rows_done(p, OUT_LAG)
        tap_exchange.wait_recv()
        tap_sum[...] = tap_in[...]

    @pl.when(is_mid)
    def _():
        for s in range(total_pieces, total_pieces + B_LAG):
            if s - A_LAG < total_pieces:
                stage_a(s - A_LAG)
            if s == total_pieces:
                tap_first()
            if s == total_pieces + A_LAG:
                tap_part.wait_recv()
                tap_two[...] = tap_two[...] + tap_out[...]
                tap_exchange.start()
                input_finish()
            stage_b((s - B_LAG) // slots, (s - B_LAG) % slots)
            rows_done(s - B_LAG, B_LAG)
        tap_exchange.wait_recv()
        tap_sum[...] = tap_two[...] + tap_in[...]
        tap_total.start()

    for c in range(chunks):
        for i in range(per):
            lane = (c * per + i) * LANES
            taps_out_ref[:, lane : lane + LANES] = tap_sum[i, c * KW : (c + 1) * KW, :]

    @pl.loop(0, chunks * 3)
    def _(n):
        c, tensor = n // 3, lax.rem(n, 3)
        for k in range(n_fs - 1):
            rs_copy(c, tensor, k).wait_send()
        for step, owner in ((0, f), (1, f), (2, across), (3, beside)):
            s = n * 4
            size = own_rows if step < 2 else own_rows // 2
            ref = g_all.at[c, pl.ds(0, size), pl.ds(0, LANES)]
            remote(ref, ref, ag_send.at[s + step], ag_recv.at[s + step], {"fs": beside}).wait_send()

    tap_part.wait_send()

    @pl.loop(0, total_pieces)
    def _(p):
        part_copy(p).wait_send()

        @pl.when(is_mid)
        def _():
            total_copy(p, tot).wait_send()

    for copy in fs_rows:
        copy.wait()
    rows_down_ref[...] = rows_d[...] + (rows_fs[0] + rows_fs[1] + rows_fs[2])
    tp_rows.wait()
    rows_gu_ref[...] = rows_gu[...] + rows_tp[...]

    @pl.when(is_mid)
    def _():
        tap_total.wait_send()


def finish_kernel(
    gate, up, down, in_grad, taps, rows_gu, rows_d,
    gate_out, up_out, down_out, in_grad_out, taps_out, rows_gate_out, rows_up_out, rows_down_out,
    wide_gate, wide_up, wide_down, sems,
):
    rows = CW
    copies = []
    for src, wide, dst in ((gate, wide_gate, gate_out), (up, wide_up, up_out), (down, wide_down, down_out)):
        for i in range(src.shape[0] // rows):
            at = pl.ds(i * rows, rows)
            wide[at, :] = src[at, :].astype(jnp.float32)
            copy = pltpu.make_async_copy(wide.at[at], dst.at[at], sems.at[len(copies)])
            copy.start()
            copies.append(copy)
    in_grad_out[...] = in_grad[...]
    taps_out[...] = taps[...]
    groups = rows_gate_out.shape[0] // LANES
    for i in range(groups):
        rows_gate_out[pl.ds(i * LANES, LANES)] = rows_gu[i]
        rows_up_out[pl.ds(i * LANES, LANES)] = rows_gu[groups + i]
    for i in range(rows_down_out.shape[0] // LANES):
        rows_down_out[pl.ds(i * LANES, LANES)] = rows_d[i]
    for copy in copies:
        copy.wait()


def fits(shape, inputs, w_gate):
    n_rep, n_fs, n_tp = shape["rep"], shape["fs"], shape["tp"]
    tok, feat = inputs.shape
    return (
        n_rep == 4 and n_fs == 4 and n_tp == 2 and feat == 2 * CW and 2 * CW <= w_gate.shape[1]
        and w_gate.shape[1] % CW == 0 and w_gate.shape[1] <= 1536 and tok % LANES == 0 and tok <= 512
    )


def fused_shards(shape, inputs, w_gate, w_up, conv_taps, w_down, out_grad):
    if not fits(shape, inputs, w_gate):
        return shards(inputs, w_gate, w_up, conv_taps, w_down, out_grad)
    n_rep, n_fs = shape["rep"], shape["fs"]
    tok, feat = inputs.shape
    hid = w_gate.shape[1]
    cw = CW
    chunks = hid // cw
    subs = feat // cw
    per = cw // LANES
    pieces = chunks * 3 * subs
    span = tok // 2 + HALO
    bf16, f32 = jnp.bfloat16, jnp.float32
    vmem = pl.BlockSpec(memory_space=pltpu.VMEM)
    hbm = pl.BlockSpec(memory_space=pltpu.HBM)
    hops = chunks * 3 * (n_fs - 1)
    dma = pltpu.SemaphoreType.DMA
    local = pltpu.VMEM
    whole = jax.ShapeDtypeStruct
    in_grad, down, gate, up, taps, rows_gu, rows_d = pl.pallas_call(
        functools.partial(layer_kernel, n_rep, n_fs),
        out_shape=(
            local((tok // 2, feat), bf16),
            local((hid, feat), bf16),
            local((feat, hid), bf16),
            local((feat, hid), bf16),
            local((KW, hid), f32),
            local((2 * subs * per, LANES), f32),
            local((chunks * per, LANES), f32),
        ),
        in_specs=[hbm, hbm, hbm, vmem, hbm, hbm],
        out_specs=(vmem,) * 7,
        scratch_shapes=[
            local((tok, feat), bf16),
            local((feat, hid), bf16),
            local((feat, hid), bf16),
            local((hid, feat), bf16),
            local((tok, feat), bf16),
            local((subs, cw, tok), bf16),
            local((chunks, 3, n_fs, span, LANES), bf16),
            local((chunks, 3, n_fs - 1, span, LANES), bf16),
            local((4, span, LANES), f32),
            local((chunks, cw, tok), bf16),
            local((chunks, tok, cw), bf16),
            local((chunks, tok, cw), bf16),
            local((RING, cw, cw), f32),
            local((pieces, cw, cw), bf16),
            local((pieces, cw, cw), bf16),
            local((pieces, cw, cw), bf16),
            local((pieces, cw, cw), bf16),
            local((tok, feat), f32),
            local((tok, feat), bf16),
            local((tok // 2, feat), bf16),
            local((n_fs, chunks * KW, LANES), f32),
            local((per, chunks * KW, LANES), f32),
            local((per, chunks * KW, LANES), f32),
            local((per, chunks * KW, LANES), f32),
            local((per, chunks * KW, LANES), f32),
            local((2 * subs * per, LANES), f32),
            local((chunks * per, LANES), f32),
            local((2 * subs * per, LANES), f32),
            local((n_fs - 1, chunks * per, LANES), f32),
            dma((hops,)), dma((hops,)), dma((chunks * 12,)), dma((chunks * 12,)),
            dma((pieces,)), dma((pieces,)), dma((pieces,)), dma((pieces,)), dma((8,)),
            dma((4 * (n_fs - 1) + 8,)),
        ],
        compiler_params=pltpu.CompilerParams(
            collective_id=0, has_side_effects=True, vmem_limit_bytes=50 * 1024 * 1024
        ),
    )(inputs, w_gate, w_up, conv_taps, w_down, out_grad)
    anywhere = pl.BlockSpec(memory_space=pl.ANY)
    copies = (2 * feat + hid) // cw
    gate, up, down, in_grad, taps, rows_gate, rows_up, rows_down = pl.pallas_call(
        finish_kernel,
        out_shape=(
            whole((feat, hid), f32), whole((feat, hid), f32), whole((hid, feat), f32),
            whole((tok // 2, feat), bf16), whole((KW, hid), f32),
            whole((feat,), f32), whole((feat,), f32), whole((hid,), f32),
        ),
        in_specs=[vmem] * 7,
        out_specs=(anywhere,) * 3 + (vmem,) * 5,
        scratch_shapes=[
            local((feat, hid), f32), local((feat, hid), f32), local((hid, feat), f32), dma((copies,)),
        ],
        compiler_params=pltpu.CompilerParams(vmem_limit_bytes=24 * 1024 * 1024),
    )(gate, up, down, in_grad, taps, rows_gu, rows_d)
    return (in_grad, gate, up, down, taps, rows_gate, rows_up, rows_down)


def solution(mesh):
    return jax.shard_map(
        functools.partial(fused_shards, dict(mesh.shape)),
        mesh=mesh,
        in_specs=(
            P("rep", "fs"),
            P("fs", "tp"),
            P("fs", "tp"),
            P(None, "tp"),
            P("tp", "fs"),
            P("rep", "fs"),
        ),
        out_specs=(
            P(("rep", "tp"), "fs"),
            P("fs", "tp"),
            P("fs", "tp"),
            P("tp", "fs"),
            P(None, "tp"),
            P("fs"),
            P("fs"),
            P("tp"),
        ),
        check_vma=False,
    )
```

```python
import functools

import jax
import jax.numpy as jnp
from jax import lax
from jax.experimental import pallas as pl
from jax.experimental.pallas import tpu as pltpu
from jax.sharding import PartitionSpec as P

KW = 3


def shift_down(values, lag_rows):
    if lag_rows == 0:
        return values
    padding = jnp.zeros_like(values[:lag_rows])
    return jnp.concatenate([padding, values[:-lag_rows]], axis=0)


def shift_up(values, lag_rows):
    if lag_rows == 0:
        return values
    padding = jnp.zeros_like(values[:lag_rows])
    return jnp.concatenate([values[lag_rows:], padding], axis=0)


def contract(left, right, left_dim, right_dim):
    return lax.dot_general(
        left, right, (((left_dim,), (right_dim,)), ((), ())), preferred_element_type=jnp.float32
    )


def row_norms(grad_gate, grad_up, grad_down):
    gate_rows = jnp.sum(grad_gate * grad_gate, axis=1)
    up_rows = jnp.sum(grad_up * grad_up, axis=1)
    down_rows = jnp.sum(grad_down * grad_down, axis=1)
    gate_rows, up_rows = lax.psum((gate_rows, up_rows), "tp")
    down_rows = lax.psum(down_rows, "fs")
    return (gate_rows, up_rows, down_rows)


def shards(inputs, w_gate, w_up, conv_taps, w_down, out_grad):
    tap_weights = conv_taps.astype(jnp.float32)
    gate_part = jnp.dot(inputs, w_gate, preferred_element_type=jnp.float32)
    up_part = jnp.dot(inputs, w_up, preferred_element_type=jnp.float32)
    act_part = contract(out_grad, w_down, 1, 1)
    gate_sum, up_sum, act_sum = (
        lax.psum(gate_part.astype(jnp.bfloat16), "fs").astype(jnp.float32),
        lax.psum(up_part.astype(jnp.bfloat16), "fs").astype(jnp.float32),
        lax.psum(act_part.astype(jnp.bfloat16), "fs").astype(jnp.float32),
    )
    gate_pre = gate_sum.astype(jnp.bfloat16)
    up_val = up_sum.astype(jnp.bfloat16)
    act_grad = act_sum.astype(jnp.bfloat16)
    gate_float = gate_pre.astype(jnp.float32)
    up_float = up_val.astype(jnp.float32)
    act_float = act_grad.astype(jnp.float32)
    shifted = [shift_down(gate_float, KW - 1 - tap_index) for tap_index in range(KW)]
    pre_act = tap_weights[0] * shifted[0]
    for tap_index in range(1, KW):
        pre_act = pre_act + tap_weights[tap_index] * shifted[tap_index]
    sigmoid_pre = jax.nn.sigmoid(pre_act)
    hidden = (pre_act * sigmoid_pre * up_float).astype(jnp.bfloat16)
    up_grad = (act_float * pre_act * sigmoid_pre).astype(jnp.bfloat16)
    pre_grad = act_float * up_float * sigmoid_pre * (1.0 + pre_act * (1.0 - sigmoid_pre))
    gate_acc = tap_weights[0] * shift_up(pre_grad, KW - 1)
    for tap_index in range(1, KW):
        gate_acc = gate_acc + tap_weights[tap_index] * shift_up(pre_grad, KW - 1 - tap_index)
    gate_grad = gate_acc.astype(jnp.bfloat16)
    gate_rows = gate_grad
    up_rows = up_grad
    in_grad = lax.psum_scatter(
        (contract(gate_rows, w_gate, 1, 1) + contract(up_rows, w_up, 1, 1)).astype(jnp.bfloat16),
        "tp",
        scatter_dimension=0,
        tiled=True,
    )
    grad_gate = contract(inputs, gate_grad, 0, 0)
    grad_up = contract(inputs, up_grad, 0, 0)
    grad_down = contract(hidden, out_grad, 0, 0)
    grad_taps = jnp.stack(
        [jnp.sum(shifted[tap_index] * pre_grad, axis=0) for tap_index in range(KW)]
    )
    grad_gate, grad_up, grad_down, grad_taps = (
        lax.psum(grad_gate.astype(jnp.bfloat16), "rep").astype(jnp.float32),
        lax.psum(grad_up.astype(jnp.bfloat16), "rep").astype(jnp.float32),
        lax.psum(grad_down.astype(jnp.bfloat16), "rep").astype(jnp.float32),
        lax.psum(grad_taps.astype(jnp.bfloat16), "rep").astype(jnp.float32),
    )
    gate_rows, up_rows, down_rows = row_norms(grad_gate, grad_up, grad_down)
    weight_grads = (grad_gate, grad_up, grad_down, grad_taps, gate_rows, up_rows, down_rows)
    grad_gate, grad_up, grad_down, grad_taps, gate_rows, up_rows, down_rows = weight_grads
    return (in_grad, grad_gate, grad_up, grad_down, grad_taps, gate_rows, up_rows, down_rows)


LANES = 128
CW = 256
HALO = 16
A_LAG = 0
B_LAG = 3
OUT_LAG = 18
RING = 2
WIDE = 4
KEEP = 24
MESH_ID = pl.DeviceIdType.MESH

STEPS = (
    (("grads", 0, 0), ("gather", 0, 1), ("reduce", 1, 0)),
    (("reduce", 1, 1), ("gather", 0, 2)),
    (),
    (("combine", 1, 0), ("combine", 1, 1), ("forward", 0, 2), ("reduce", 1, 2)),
    (("hidden", 1, 0),),
    (("combine", 1, 2),),
)


def layer_kernel(
    n_rep, n_fs,
    x_hbm, wg_hbm, wu_hbm, taps_ref, wd_hbm, og_hbm,
    in_grad_out, down_ref, gate_ref, up_ref, taps_out, rows_gu_out, rows_down_out,
    x_ref, wg_ref, wu_ref, wd_ref, og_ref,
    xt, send_part, recv_part, pair_part, held, h_all, g_all, u_all, ring, wide, part, from_out, from_in, tot,
    acc, ig_send, ig_recv, in_grad_ref, taps_out_ref, rows_gu_ref, rows_down_ref, tap_all, tap_two, tap_out, tap_in, tap_sum, rows_gu, rows_d, rows_tp, rows_fs,
    rs_send, rs_recv, ag_send, ag_recv, a_send, out_recv, in_recv, b_send, wide_sem, out_sem, loc_sem, misc,
):
    tok, feat = x_ref.shape
    cw = CW
    chunks = wg_ref.shape[1] // cw
    subs = feat // cw
    own_rows = tok // 2
    span = own_rows + HALO
    slots = 3 * subs
    total_pieces = chunks * slots
    per = cw // LANES
    f32, bf16 = jnp.float32, jnp.bfloat16
    r = lax.axis_index("rep")
    f = lax.axis_index("fs")
    t = lax.axis_index("tp")
    half_rep = n_rep // 2
    is_left = r < half_rep
    toward = jnp.where(is_left, r + 1, r - 1)
    outward = jnp.where(is_left, r - 1, r + 1)
    is_end = jnp.logical_or(r == 0, r == n_rep - 1)
    is_mid = jnp.logical_not(is_end)
    beside = f + 1 - 2 * lax.rem(f, 2)
    across = lax.rem(f + 2, 4)
    corner = lax.rem(beside + 2, 4)
    peers = [beside, across, corner]
    side = lax.rem(f, 2)
    top = f // 2
    own_cols = pl.ds(pl.multiple_of(side * LANES, LANES), LANES)
    own_toks = pl.ds(pl.multiple_of(top * own_rows, own_rows), own_rows)

    barrier = pltpu.get_barrier_semaphore()
    for k in range(n_fs - 1):
        pl.semaphore_signal(barrier, inc=1, device_id={"fs": peers[k]}, device_id_type=MESH_ID)
    pl.semaphore_signal(barrier, inc=1, device_id={"tp": 1 - t}, device_id_type=MESH_ID)
    pl.semaphore_signal(barrier, inc=1, device_id={"rep": toward}, device_id_type=MESH_ID)

    @pl.when(is_mid)
    def _():
        pl.semaphore_signal(barrier, inc=1, device_id={"rep": outward}, device_id_type=MESH_ID)

    loads = []

    def load(src, dst):
        copy = pltpu.make_async_copy(src, dst, loc_sem.at[len(loads)])
        copy.start()
        loads.append(copy)

    first = slice(0, cw)
    load(x_hbm, x_ref)
    load(wg_hbm.at[:, first], wg_ref.at[:, first])
    load(wu_hbm.at[:, first], wu_ref.at[:, first])
    load(og_hbm, og_ref)
    load(wd_hbm.at[first], wd_ref.at[first])
    if chunks > 1:
        rest = slice(cw, chunks * cw)
        load(wg_hbm.at[:, rest], wg_ref.at[:, rest])
        load(wu_hbm.at[:, rest], wu_ref.at[:, rest])
        load(wd_hbm.at[rest], wd_ref.at[rest])

    def remote(src, dst, send, recv, device):
        return pltpu.make_async_remote_copy(
            src_ref=src, dst_ref=dst, send_sem=send, recv_sem=recv,
            device_id=device, device_id_type=MESH_ID,
        )

    def chunk_cols(c):
        if isinstance(c, int):
            return slice(c * cw, (c + 1) * cw)
        return pl.ds(pl.multiple_of(c * cw, cw), cw)

    cut = recv_part.shape[3]
    halves = (slice(0, cut), slice(cut, span))

    def rs_copy(c, tensor, n):
        s = (lax.rem(c, 2) * 3 + tensor) * 6 + n
        side_of = n % 2
        near, far = (beside, across) if side_of == 0 else (across, beside)
        rows = halves[side_of]
        size = rows.stop - rows.start
        owner = corner if n < 2 else near
        target = near if n < 4 else far
        if n < 4:
            src = send_part.at[c, tensor, owner, rows]
        else:
            src = pair_part.at[c, tensor, side_of, 0:size]
        return remote(
            src, recv_part.at[c, tensor, n, 0:size], rs_send.at[n], rs_recv.at[s], {"fs": target}
        )

    def product(c, tensor):
        cols = chunk_cols(c)
        if tensor == 0:
            value = jnp.dot(x_ref[...], wg_ref[:, cols], preferred_element_type=f32)
        elif tensor == 1:
            value = jnp.dot(x_ref[...], wu_ref[:, cols], preferred_element_type=f32)
        else:
            value = contract(og_ref[...], wd_ref[cols, :], 1, 1)
        value = value.astype(bf16)
        for g in range(n_fs):
            row = (g // 2) * (own_rows - HALO)
            lane = (g % 2) * LANES
            send_part[c, tensor, g] = value[row : row + span, lane : lane + LANES]

    def reduce_send(c, tensor):
        for n in range(4):
            rs_copy(c, tensor, n).start()

    def reduce_start(c, tensor):
        product(c, tensor)
        reduce_send(c, tensor)

    def combine(c, tensor):
        for n in range(2):
            rows = halves[n]
            size = rows.stop - rows.start
            rs_copy(c, tensor, n).wait_recv()
            mine = send_part[c, tensor, across if n == 0 else beside, rows]
            pair_part[c, tensor, n, 0:size] = (
                mine.astype(f32) + recv_part[c, tensor, n, 0:size].astype(f32)
            ).astype(bf16)
            rs_copy(c, tensor, 4 + n).start()

    def reduced(c, tensor):
        parts = []
        for n in range(2):
            rows = halves[n]
            size = rows.stop - rows.start
            rs_copy(c, tensor, 2 + n).wait_recv()
            value = send_part[c, tensor, f, rows].astype(f32) + recv_part[c, tensor, 2 + n, 0:size].astype(f32)
            rs_copy(c, tensor, 4 + n).wait_recv()
            parts.append(value + recv_part[c, tensor, 4 + n, 0:size].astype(f32))
        return jnp.concatenate(parts, axis=0).astype(bf16).astype(f32)

    def block(c, tensor, owner, part_of=None):
        col = lax.rem(owner, 2) * LANES
        row = (owner // 2) * own_rows
        if tensor == 0:
            size = LANES if part_of is None else LANES // 2
            start = col + (0 if part_of is None else part_of * size)
            return h_all.at[
                c, pl.ds(pl.multiple_of(start, size), size), pl.ds(pl.multiple_of(row, own_rows), own_rows)
            ]
        size = own_rows if part_of is None else own_rows // 2
        start = row + (0 if part_of is None else part_of * size)
        ref = g_all if tensor == 1 else u_all
        return ref.at[c, pl.ds(pl.multiple_of(start, size), size), pl.ds(pl.multiple_of(col, LANES), LANES)]

    def ag_copy(c, tensor, step, owner):
        s = (lax.rem(c, 2) * 3 + tensor) * 4
        if step == 0:
            ref, slot, target = block(c, tensor, owner), 0, beside
        elif step == 1:
            ref, slot, target = block(c, tensor, owner), 1, across
        elif step == 2:
            ref, slot, target = block(c, tensor, owner, 1), 2, beside
        else:
            ref, slot, target = block(c, tensor, owner, 0), 3, across
        return remote(ref, ref, ag_send.at[slot], ag_recv.at[s + slot], {"fs": target})

    def corner_copy(c, tensor, owner):
        ref, s = block(c, tensor, owner), (lax.rem(c, 2) * 3 + tensor) * 4 + 2
        return remote(ref, ref, ag_send.at[2], ag_recv.at[s], {"fs": corner})

    def gather_start(c, tensor):
        for step in (0, 1):
            ag_copy(c, tensor, step, f).start()
        if tensor < 2:
            corner_copy(c, tensor, f).start()

    def forward(c, tensor):
        ag_copy(c, tensor, 0, beside).wait_recv()
        ag_copy(c, tensor, 3, beside).start()
        ag_copy(c, tensor, 1, across).wait_recv()
        ag_copy(c, tensor, 2, across).start()

    def gathered(c, tensor):
        if tensor < 2:
            ag_copy(c, tensor, 0, beside).wait_recv()
            ag_copy(c, tensor, 1, across).wait_recv()
            corner_copy(c, tensor, corner).wait_recv()
        else:
            ag_copy(c, tensor, 2, corner).wait_recv()
            ag_copy(c, tensor, 3, corner).wait_recv()

    def own(value):
        return jnp.where(top == 0, value[:own_rows], value[HALO:])

    row_ids = lax.broadcasted_iota(jnp.int32, (span, LANES), 0)

    def down(value, lag):
        if lag == 0:
            return value
        return jnp.where(row_ids >= lag, pltpu.roll(value, lag, 0), 0.0)

    def up(value, lag):
        if lag == 0:
            return value
        return jnp.where(row_ids < span - lag, pltpu.roll(value, span - lag, 0), 0.0)

    def own_weights(c):
        cols = pl.ds(pl.multiple_of(c * cw + side * LANES, LANES), LANES)
        return taps_ref[:, cols].astype(f32)

    def hidden_step(c):
        weights = own_weights(c)
        gate = reduced(c, 0)
        pre = weights[0:1] * down(gate, KW - 1)
        for j in range(1, KW):
            pre = pre + weights[j : j + 1] * down(gate, KW - 1 - j)
        sig = 1.0 / (1.0 + jnp.exp(-pre))
        up_val = reduced(c, 1)
        h_all[c, own_cols, own_toks] = own(pre * sig * up_val).T.astype(bf16)
        gather_start(c, 0)
        held[0] = gate
        held[1] = up_val
        held[2] = pre
        held[3] = sig

    def grads_step(c):
        weights = own_weights(c)
        gate, up_val, pre, sig = held[0], held[1], held[2], held[3]
        act = reduced(c, 2)
        pre_grad = act * up_val * sig * (1.0 + pre * (1.0 - sig))
        grad = weights[0:1] * up(pre_grad, KW - 1)
        for j in range(1, KW):
            grad = grad + weights[j : j + 1] * up(pre_grad, KW - 1 - j)
        g_all[c, own_toks, own_cols] = own(grad).astype(bf16)
        u_all[c, own_toks, own_cols] = own(act * (pre * sig)).astype(bf16)
        for j in range(KW):
            tap_all[f, pl.ds(c * KW + j, 1), :] = jnp.sum(
                own(down(gate, KW - 1 - j) * pre_grad), axis=0, keepdims=True
            )

    def half_rows(h):
        return slice(h * LANES, (h + 1) * LANES)

    def part_copy(p, h):
        rows = half_rows(h)
        s = lax.rem(p * per + h, KEEP)
        return remote(part.at[p, rows], from_out.at[p, rows], a_send.at[0], out_recv.at[s], {"rep": toward})

    def exchange_copy(p, h):
        rows = half_rows(h)
        s = lax.rem(p * per + h, KEEP)
        return remote(part.at[p, rows], from_in.at[p, rows], a_send.at[0], in_recv.at[s], {"rep": toward})

    def total_copy(p, h):
        rows = half_rows(h)
        s = lax.rem(p * per + h, KEEP)
        return remote(tot.at[p, rows], from_in.at[p, rows], b_send.at[0], in_recv.at[s], {"rep": outward})

    def piece_rows(base, h):
        if isinstance(base, int):
            return slice(base + h * LANES, base + (h + 1) * LANES)
        return pl.ds(pl.multiple_of(base + h * LANES, LANES), LANES)

    def place(c, s, h):
        tensor, q = s // subs, s % subs
        slot = (s * per + h) % WIDE
        if tensor == 0:
            dst = down_ref.at[piece_rows(c * cw, h), q * cw : (q + 1) * cw]
        elif tensor == 1:
            dst = gate_ref.at[piece_rows(q * cw, h), chunk_cols(c)]
        else:
            dst = up_ref.at[piece_rows(q * cw, h), chunk_cols(c)]
        return pltpu.make_async_copy(wide.at[slot], dst, wide_sem.at[slot])

    def finished(c, s, h, value):
        tensor, q = s // subs, s % subs
        value = value.astype(f32)
        slot = (s * per + h) % WIDE
        copy = place(c, s, h)
        if not isinstance(c, int):
            pl.when((c * slots + s) * per + h >= WIDE)(copy.wait)
        elif (c * slots + s) * per + h >= WIDE:
            copy.wait()
        wide[slot] = value
        copy.start()
        square = value * value
        lanes = square[:, :LANES]
        for g in range(1, cw // LANES):
            lanes = lanes + square[:, g * LANES : (g + 1) * LANES]
        row = jnp.sum(lanes.T, axis=0, keepdims=True)
        if tensor == 0:
            at = pl.ds(c * per + h, 1)
            rows_d[at, :] = row if q == 0 else rows_d[at, :] + row
        else:
            at = ((tensor - 1) * subs + q) * per + h
            rows_gu[at : at + 1, :] = rows_gu[at : at + 1, :] + row

    def stage_a(p, h):
        part_copy(p, h).wait_recv()
        rows = half_rows(h)
        part[p, rows] = (ring[lax.rem(p, RING), rows] + from_out[p, rows].astype(f32)).astype(bf16)
        exchange_copy(p, h).start()

    def stage_b(c, s, h):
        p = c * slots + s
        rows = half_rows(h)
        exchange_copy(p, h).wait_recv()
        value = (part[p, rows].astype(f32) + from_in[p, rows].astype(f32)).astype(bf16)
        tot[p, rows] = value
        total_copy(p, h).start()
        finished(c, s, h, value)

    def stage_out(c, s, h):
        p = c * slots + s
        exchange_copy(p, h).wait_recv()
        finished(c, s, h, from_in[p, half_rows(h)])

    def behind(c, s, h, lag):
        steps = slots * per
        at = s * per + h - lag
        back = (-at + steps - 1) // steps if at < 0 else 0
        at += back * steps
        return c - back, at // per, at % per, back

    def guarded(c, lowest, fn):
        if isinstance(c, int):
            if c >= lowest:
                fn()
        elif lowest <= 1:
            fn()
        else:
            pl.when(c >= lowest)(fn)

    def work(c, s):
        tensor, q = s // subs, s % subs
        p = c * slots + s
        if q == 0:
            gathered(c, tensor)
        if tensor == 0:
            value = jnp.dot(h_all[c], og_ref[:, q * cw : (q + 1) * cw], preferred_element_type=f32)
        elif tensor == 1:
            value = jnp.dot(xt[q], g_all[c], preferred_element_type=f32)
        else:
            value = jnp.dot(xt[q], u_all[c], preferred_element_type=f32)

        @pl.when(is_end)
        def _():
            for h in range(per):
                part[p, half_rows(h)] = value[half_rows(h)].astype(bf16)
                part_copy(p, h).start()
            for h in range(per):
                co, so, ho, ko = behind(c, s, h, OUT_LAG)
                guarded(c, ko, functools.partial(stage_out, co, so, ho))

        @pl.when(is_mid)
        def _():
            ring[lax.rem(p, RING)] = value
            for h in range(per):
                ca, sa, ha, ka = behind(c, s, h, A_LAG)
                guarded(c, ka, functools.partial(stage_a, ca * slots + sa, ha))
                cb, sb, hb, kb = behind(c, s, h, B_LAG)
                guarded(c, kb, functools.partial(stage_b, cb, sb, hb))

    def input_term(c):
        cols = chunk_cols(c)
        term = contract(g_all[c], wg_ref[:, cols], 1, 1) + contract(u_all[c], wu_ref[:, cols], 1, 1)
        if isinstance(c, int) and c == 0:
            acc[...] = term
        else:
            acc[...] += term

    actions = {
        "forward": forward,
        "reduce": reduce_start,
        "combine": combine,
        "hidden": lambda c, tensor: hidden_step(c),
        "grads": lambda c, tensor: grads_step(c),
        "gather": gather_start,
    }

    def run(step, c):
        name, ahead, tensor = step
        target = c + ahead
        if isinstance(c, int):
            if target < chunks:
                actions[name](target, tensor)
        elif ahead == 0:
            actions[name](target, tensor)
        else:
            pl.when(target < chunks)(lambda: actions[name](target, tensor))

    m = 2 * (n_fs - 1)
    half = tok // 2
    ig_copy = remote(
        ig_send.at[pl.ds(pl.multiple_of((1 - t) * half, half), half)], ig_recv,
        misc.at[m], misc.at[m + 1], {"tp": 1 - t},
    )
    tap_peers = [
        remote(tap_all.at[f], tap_all.at[f], misc.at[2 * k], misc.at[2 * k + 1], {"fs": peers[k]})
        for k in range(n_fs - 1)
    ]
    tap_part = remote(tap_two, tap_out, misc.at[m + 2], misc.at[m + 3], {"rep": toward})
    tap_exchange = remote(tap_two, tap_in, misc.at[m + 2], misc.at[m + 4], {"rep": toward})
    tap_total = remote(tap_sum, tap_in, misc.at[m + 5], misc.at[m + 4], {"rep": outward})
    fs_rows = [
        remote(rows_d, rows_fs.at[k], misc.at[m + 8 + 2 * k], misc.at[m + 9 + 2 * k], {"fs": peers[k]})
        for k in range(n_fs - 1)
    ]
    tp_rows = remote(rows_gu, rows_tp, misc.at[m + 6], misc.at[m + 7], {"tp": 1 - t})

    outputs = [
        pltpu.make_async_copy(src, dst, out_sem.at[n])
        for n, (src, dst) in enumerate((
            (in_grad_ref, in_grad_out), (taps_out_ref, taps_out),
            (rows_down_ref, rows_down_out), (rows_gu_ref, rows_gu_out),
        ))
    ]

    def tap_first():
        for copy in tap_peers:
            copy.wait()
        for i in range(per):
            tap_two[i] = tap_all[i] + tap_all[i + 2]
        pl.when(is_end)(tap_part.start)

    def tap_second():
        tap_part.wait_recv()
        tap_two[...] = tap_two[...] + tap_out[...]
        tap_exchange.start()

    def tap_place():
        for c in range(chunks):
            for i in range(per):
                lane = (c * per + i) * LANES
                taps_out_ref[:, lane : lane + LANES] = tap_sum[i, c * KW : (c + 1) * KW, :]
        outputs[1].start()

    def input_start():
        ig_send[...] = acc[...].astype(bf16)
        ig_copy.start()

    def input_finish():
        ig_copy.wait()
        in_grad_ref[...] = (
            ig_send[pl.ds(pl.multiple_of(t * half, half), half), :].astype(f32) + ig_recv[...].astype(f32)
        ).astype(bf16)
        outputs[0].start()

    def body(c, last=False):
        for s in range(slots):
            if s > 0 or not isinstance(c, int) or c > 0:
                for step in STEPS[s]:
                    run(step, c)
            if last and s == 1:
                for copy in tap_peers:
                    copy.start()
            if last and s == 3:
                tap_first()
            if last and s == slots - 2:
                pl.when(is_mid)(tap_second)
            work(c, s)
        input_term(c)

    loads[0].wait()
    loads[1].wait()
    product(0, 0)
    loads[2].wait()
    product(0, 1)
    pl.semaphore_wait(barrier, n_fs + 1 + jnp.where(is_mid, 1, 0))
    reduce_send(0, 0)
    reduce_send(0, 1)
    loads[3].wait()
    loads[4].wait()
    product(0, 2)
    for q in range(subs):
        xt[q] = x_ref[:, q * cw : (q + 1) * cw].astype(f32).T.astype(bf16)
    rows_gu[...] = jnp.zeros_like(rows_gu)
    for copy in loads[5:]:
        copy.wait()
    combine(0, 0)
    combine(0, 1)
    reduce_send(0, 2)
    if chunks > 1:
        product(1, 0)
    hidden_step(0)
    combine(0, 2)
    grads_step(0)
    gather_start(0, 1)
    if chunks > 1:
        reduce_send(1, 0)
    body(0)

    @pl.loop(1, chunks - 1)
    def _(c):
        body(c)

    body(chunks - 1, last=True)
    input_start()
    down_last = total_pieces - slots + subs - 1

    steps = total_pieces * per

    @pl.when(is_end)
    def _():
        for k in range(steps - OUT_LAG, steps):
            p = k // per
            if k == steps - 1:
                input_finish()
                tap_exchange.wait_recv()
                tap_sum[...] = tap_in[...]
                tap_place()
            stage_out(p // slots, p % slots, k % per)
            if k == max(steps - OUT_LAG, (down_last + 1) * per - 1):
                for copy in fs_rows:
                    copy.start()

    @pl.when(is_mid)
    def _():
        for copy in fs_rows:
            copy.start()
        for k in range(steps, steps + B_LAG):
            if k - A_LAG < steps:
                stage_a((k - A_LAG) // per, (k - A_LAG) % per)
            p = (k - B_LAG) // per
            stage_b(p // slots, p % slots, (k - B_LAG) % per)
            if k == steps:
                tap_exchange.wait_recv()
                tap_sum[...] = tap_two[...] + tap_in[...]
                tap_total.start()
                input_finish()
                tap_place()

    tp_rows.start()

    def all_sent(ref, sem):
        remote(ref, ref, sem, sem, {"tp": 1 - t}).wait_send()

    for n in range(6):
        rows = halves[n % 2]
        all_sent(recv_part.at[:, :, n, 0 : rows.stop - rows.start], rs_send.at[n])
    columns = h_all.shape[1]
    for slot, quarters in ((0, 12), (1, 12), (2, 10), (3, 2)):
        all_sent(h_all.at[:, 0 : columns * quarters // 16], ag_send.at[slot])
    all_sent(part, a_send.at[0])
    tap_part.wait_send()

    @pl.when(is_mid)
    def _():
        all_sent(tot, b_send.at[0])

    for k in range(steps - WIDE, steps):
        p = k // per
        place(p // slots, p % slots, k % per).wait()
    for copy in fs_rows:
        copy.wait()
    rows_down_ref[...] = rows_d[...] + (rows_fs[0] + rows_fs[1] + rows_fs[2])
    outputs[2].start()
    tp_rows.wait()
    rows_gu_ref[...] = rows_gu[...] + rows_tp[...]
    outputs[3].start()
    for copy in outputs:
        copy.wait()

    @pl.when(is_mid)
    def _():
        tap_total.wait_send()


def finish_kernel(
    gate, up, down, in_grad, taps, rows_gu, rows_d,
    gate_out, up_out, down_out, in_grad_out, taps_out, rows_gate_out, rows_up_out, rows_down_out,
    sems,
):
    copies = []
    for src, dst in ((gate, gate_out), (up, up_out), (down, down_out)):
        copy = pltpu.make_async_copy(src, dst, sems.at[len(copies)])
        copy.start()
        copies.append(copy)
    in_grad_out[...] = in_grad[...]
    taps_out[...] = taps[...]
    groups = rows_gate_out.shape[0] // LANES
    for i in range(groups):
        rows_gate_out[pl.ds(i * LANES, LANES)] = rows_gu[i]
        rows_up_out[pl.ds(i * LANES, LANES)] = rows_gu[groups + i]
    for i in range(rows_down_out.shape[0] // LANES):
        rows_down_out[pl.ds(i * LANES, LANES)] = rows_d[i]
    for copy in copies:
        copy.wait()


def fits(shape, inputs, w_gate):
    n_rep, n_fs, n_tp = shape["rep"], shape["fs"], shape["tp"]
    tok, feat = inputs.shape
    return (
        n_rep == 4 and n_fs == 4 and n_tp == 2 and feat == 2 * CW and 3 * CW <= w_gate.shape[1]
        and w_gate.shape[1] % CW == 0 and w_gate.shape[1] <= 1536 and tok % (2 * LANES) == 0 and tok <= 512
    )


def fused_shards(shape, inputs, w_gate, w_up, conv_taps, w_down, out_grad):
    if not fits(shape, inputs, w_gate):
        return shards(inputs, w_gate, w_up, conv_taps, w_down, out_grad)
    n_rep, n_fs = shape["rep"], shape["fs"]
    tok, feat = inputs.shape
    hid = w_gate.shape[1]
    cw = CW
    chunks = hid // cw
    subs = feat // cw
    per = cw // LANES
    pieces = chunks * 3 * subs
    span = tok // 2 + HALO
    cut = -(-span // (2 * HALO)) * HALO
    bf16, f32 = jnp.bfloat16, jnp.float32
    vmem = pl.BlockSpec(memory_space=pltpu.VMEM)
    hbm = pl.BlockSpec(memory_space=pltpu.HBM)
    anywhere = pl.BlockSpec(memory_space=pl.ANY)
    dma = pltpu.SemaphoreType.DMA
    local = pltpu.VMEM
    whole = jax.ShapeDtypeStruct
    in_grad, down, gate, up, taps, rows_gu, rows_d = pl.pallas_call(
        functools.partial(layer_kernel, n_rep, n_fs),
        out_shape=(
            local((tok // 2, feat), bf16),
            local((hid, feat), f32),
            local((feat, hid), f32),
            local((feat, hid), f32),
            local((KW, hid), f32),
            local((2 * subs * per, LANES), f32),
            local((chunks * per, LANES), f32),
        ),
        in_specs=[hbm, hbm, hbm, vmem, hbm, hbm],
        out_specs=(anywhere,) * 7,
        scratch_shapes=[
            local((tok, feat), bf16),
            local((feat, hid), bf16),
            local((feat, hid), bf16),
            local((hid, feat), bf16),
            local((tok, feat), bf16),
            local((subs, cw, tok), bf16),
            local((chunks, 3, n_fs, span, LANES), bf16),
            local((chunks, 3, 6, cut, LANES), bf16),
            local((chunks, 3, 2, cut, LANES), bf16),
            local((4, span, LANES), f32),
            local((chunks, cw, tok), bf16),
            local((chunks, tok, cw), bf16),
            local((chunks, tok, cw), bf16),
            local((RING, cw, cw), f32),
            local((WIDE, LANES, cw), f32),
            local((pieces, cw, cw), bf16),
            local((pieces, cw, cw), bf16),
            local((pieces, cw, cw), bf16),
            local((pieces, cw, cw), bf16),
            local((tok, feat), f32),
            local((tok, feat), bf16),
            local((tok // 2, feat), bf16),
            local((tok // 2, feat), bf16),
            local((KW, hid), f32),
            local((2 * subs * per, LANES), f32),
            local((chunks * per, LANES), f32),
            local((n_fs, chunks * KW, LANES), f32),
            local((per, chunks * KW, LANES), f32),
            local((per, chunks * KW, LANES), f32),
            local((per, chunks * KW, LANES), f32),
            local((per, chunks * KW, LANES), f32),
            local((2 * subs * per, LANES), f32),
            local((chunks * per, LANES), f32),
            local((2 * subs * per, LANES), f32),
            local((n_fs - 1, chunks * per, LANES), f32),
            dma((6,)), dma((36,)), dma((4,)), dma((24,)),
            dma((1,)), dma((KEEP,)), dma((KEEP,)), dma((1,)), dma((WIDE,)), dma((4,)), dma((8,)),
            dma((4 * (n_fs - 1) + 8,)),
        ],
        compiler_params=pltpu.CompilerParams(
            collective_id=0, has_side_effects=True, vmem_limit_bytes=50 * 1024 * 1024
        ),
    )(inputs, w_gate, w_up, conv_taps, w_down, out_grad)
    gate, up, down, in_grad, taps, rows_gate, rows_up, rows_down = pl.pallas_call(
        finish_kernel,
        out_shape=(
            whole((feat, hid), f32), whole((feat, hid), f32), whole((hid, feat), f32),
            whole((tok // 2, feat), bf16), whole((KW, hid), f32),
            whole((feat,), f32), whole((feat,), f32), whole((hid,), f32),
        ),
        in_specs=[anywhere] * 3 + [vmem] * 4,
        out_specs=(anywhere,) * 3 + (vmem,) * 5,
        scratch_shapes=[dma((3,))],
        compiler_params=pltpu.CompilerParams(vmem_limit_bytes=24 * 1024 * 1024),
    )(gate, up, down, in_grad, taps, rows_gu, rows_d)
    return (in_grad, gate, up, down, taps, rows_gate, rows_up, rows_down)


def solution(mesh):
    return jax.shard_map(
        functools.partial(fused_shards, dict(mesh.shape)),
        mesh=mesh,
        in_specs=(
            P("rep", "fs"),
            P("fs", "tp"),
            P("fs", "tp"),
            P(None, "tp"),
            P("tp", "fs"),
            P("rep", "fs"),
        ),
        out_specs=(
            P(("rep", "tp"), "fs"),
            P("fs", "tp"),
            P("fs", "tp"),
            P("tp", "fs"),
            P(None, "tp"),
            P("fs"),
            P("fs"),
            P("tp"),
        ),
        check_vma=False,
    )
```

```python
import functools

import jax
import jax.numpy as jnp
from jax import lax
from jax.experimental import pallas as pl
from jax.experimental.pallas import tpu as pltpu
from jax.sharding import PartitionSpec as P

KW = 3


def shift_down(values, lag_rows):
    if lag_rows == 0:
        return values
    padding = jnp.zeros_like(values[:lag_rows])
    return jnp.concatenate([padding, values[:-lag_rows]], axis=0)


def shift_up(values, lag_rows):
    if lag_rows == 0:
        return values
    padding = jnp.zeros_like(values[:lag_rows])
    return jnp.concatenate([values[lag_rows:], padding], axis=0)


def contract(left, right, left_dim, right_dim):
    return lax.dot_general(
        left, right, (((left_dim,), (right_dim,)), ((), ())), preferred_element_type=jnp.float32
    )


def row_norms(grad_gate, grad_up, grad_down):
    gate_rows = jnp.sum(grad_gate * grad_gate, axis=1)
    up_rows = jnp.sum(grad_up * grad_up, axis=1)
    down_rows = jnp.sum(grad_down * grad_down, axis=1)
    gate_rows, up_rows = lax.psum((gate_rows, up_rows), "tp")
    down_rows = lax.psum(down_rows, "fs")
    return (gate_rows, up_rows, down_rows)


def shards(inputs, w_gate, w_up, conv_taps, w_down, out_grad):
    tap_weights = conv_taps.astype(jnp.float32)
    gate_part = jnp.dot(inputs, w_gate, preferred_element_type=jnp.float32)
    up_part = jnp.dot(inputs, w_up, preferred_element_type=jnp.float32)
    act_part = contract(out_grad, w_down, 1, 1)
    gate_sum, up_sum, act_sum = (
        lax.psum(gate_part.astype(jnp.bfloat16), "fs").astype(jnp.float32),
        lax.psum(up_part.astype(jnp.bfloat16), "fs").astype(jnp.float32),
        lax.psum(act_part.astype(jnp.bfloat16), "fs").astype(jnp.float32),
    )
    gate_pre = gate_sum.astype(jnp.bfloat16)
    up_val = up_sum.astype(jnp.bfloat16)
    act_grad = act_sum.astype(jnp.bfloat16)
    gate_float = gate_pre.astype(jnp.float32)
    up_float = up_val.astype(jnp.float32)
    act_float = act_grad.astype(jnp.float32)
    shifted = [shift_down(gate_float, KW - 1 - tap_index) for tap_index in range(KW)]
    pre_act = tap_weights[0] * shifted[0]
    for tap_index in range(1, KW):
        pre_act = pre_act + tap_weights[tap_index] * shifted[tap_index]
    sigmoid_pre = jax.nn.sigmoid(pre_act)
    hidden = (pre_act * sigmoid_pre * up_float).astype(jnp.bfloat16)
    up_grad = (act_float * pre_act * sigmoid_pre).astype(jnp.bfloat16)
    pre_grad = act_float * up_float * sigmoid_pre * (1.0 + pre_act * (1.0 - sigmoid_pre))
    gate_acc = tap_weights[0] * shift_up(pre_grad, KW - 1)
    for tap_index in range(1, KW):
        gate_acc = gate_acc + tap_weights[tap_index] * shift_up(pre_grad, KW - 1 - tap_index)
    gate_grad = gate_acc.astype(jnp.bfloat16)
    gate_rows = gate_grad
    up_rows = up_grad
    in_grad = lax.psum_scatter(
        (contract(gate_rows, w_gate, 1, 1) + contract(up_rows, w_up, 1, 1)).astype(jnp.bfloat16),
        "tp",
        scatter_dimension=0,
        tiled=True,
    )
    grad_gate = contract(inputs, gate_grad, 0, 0)
    grad_up = contract(inputs, up_grad, 0, 0)
    grad_down = contract(hidden, out_grad, 0, 0)
    grad_taps = jnp.stack(
        [jnp.sum(shifted[tap_index] * pre_grad, axis=0) for tap_index in range(KW)]
    )
    grad_gate, grad_up, grad_down, grad_taps = (
        lax.psum(grad_gate.astype(jnp.bfloat16), "rep").astype(jnp.float32),
        lax.psum(grad_up.astype(jnp.bfloat16), "rep").astype(jnp.float32),
        lax.psum(grad_down.astype(jnp.bfloat16), "rep").astype(jnp.float32),
        lax.psum(grad_taps.astype(jnp.bfloat16), "rep").astype(jnp.float32),
    )
    gate_rows, up_rows, down_rows = row_norms(grad_gate, grad_up, grad_down)
    weight_grads = (grad_gate, grad_up, grad_down, grad_taps, gate_rows, up_rows, down_rows)
    grad_gate, grad_up, grad_down, grad_taps, gate_rows, up_rows, down_rows = weight_grads
    return (in_grad, grad_gate, grad_up, grad_down, grad_taps, gate_rows, up_rows, down_rows)


LANES = 128
CW = 256
HALO = 16
A_LAG = 1
B_LAG = 4
OUT_LAG = 18
RING = 2
WIDE = 4
KEEP = 24
MESH_ID = pl.DeviceIdType.MESH

STEPS = (
    (("grads", 0, 0), ("gather", 0, 1), ("reduce", 1, 0)),
    (("forward", 0, 1), ("gather", 0, 2)),
    (("combine", 1, 0), ("combine", 1, 1), ("reduce", 1, 2)),
    (("forward", 0, 2),),
    (("hidden", 1, 0), ("combine", 1, 2), ("reduce", 2, 1)),
    (("forward", 1, 0),),
)
FIRST_STEPS = ((), (("gather", 0, 2),), (), STEPS[2] + STEPS[3]) + STEPS[4:]


def layer_kernel(
    n_rep, n_fs,
    x_hbm, wg_hbm, wu_hbm, taps_ref, wd_hbm, og_hbm,
    in_grad_out, down_ref, gate_ref, up_ref, taps_out, rows_gu_out, rows_down_out,
    x_ref, wg_ref, wu_ref, wd_ref, og_ref,
    xt, send_part, recv_part, pair_part, held, h_all, g_all, u_all, ring, wide, part, from_out, from_in, tot,
    acc, ig_send, ig_recv, in_grad_ref, taps_out_ref, rows_gu_ref, rows_down_ref, tap_all, tap_two, tap_out, tap_in, tap_sum, rows_gu, rows_d, rows_tp, rows_fs,
    rs_send, rs_recv, ag_send, ag_recv, a_send, out_recv, in_recv, b_send, wide_sem, out_sem, loc_sem, go_sem, misc,
):
    tok, feat = x_ref.shape
    cw = CW
    chunks = wg_ref.shape[1] // cw
    subs = feat // cw
    own_rows = tok // 2
    span = own_rows + HALO
    slots = 3 * subs
    total_pieces = chunks * slots
    per = cw // LANES
    f32, bf16 = jnp.float32, jnp.bfloat16
    r = lax.axis_index("rep")
    f = lax.axis_index("fs")
    t = lax.axis_index("tp")
    half_rep = n_rep // 2
    is_left = r < half_rep
    toward = jnp.where(is_left, r + 1, r - 1)
    outward = jnp.where(is_left, r - 1, r + 1)
    is_end = jnp.logical_or(r == 0, r == n_rep - 1)
    is_mid = jnp.logical_not(is_end)
    beside = f + 1 - 2 * lax.rem(f, 2)
    across = lax.rem(f + 2, 4)
    corner = lax.rem(beside + 2, 4)
    peers = [beside, across, corner]
    side = lax.rem(f, 2)
    top = f // 2
    own_cols = pl.ds(pl.multiple_of(side * LANES, LANES), LANES)
    own_toks = pl.ds(pl.multiple_of(top * own_rows, own_rows), own_rows)

    barrier = pltpu.get_barrier_semaphore()
    for k in range(n_fs - 1):
        pl.semaphore_signal(barrier, inc=1, device_id={"fs": peers[k]}, device_id_type=MESH_ID)
    pl.semaphore_signal(barrier, inc=1, device_id={"tp": 1 - t}, device_id_type=MESH_ID)
    pl.semaphore_signal(barrier, inc=1, device_id={"rep": toward}, device_id_type=MESH_ID)

    @pl.when(is_mid)
    def _():
        pl.semaphore_signal(barrier, inc=1, device_id={"rep": outward}, device_id_type=MESH_ID)

    loads = []

    def load(src, dst):
        copy = pltpu.make_async_copy(src, dst, loc_sem.at[len(loads)])
        copy.start()
        loads.append(copy)

    first = slice(0, cw)
    load(x_hbm, x_ref)
    load(wg_hbm.at[:, first], wg_ref.at[:, first])
    load(wu_hbm.at[:, first], wu_ref.at[:, first])
    load(og_hbm, og_ref)
    load(wd_hbm.at[first], wd_ref.at[first])
    if chunks > 1:
        rest = slice(cw, chunks * cw)
        load(wg_hbm.at[:, rest], wg_ref.at[:, rest])
        load(wu_hbm.at[:, rest], wu_ref.at[:, rest])
        load(wd_hbm.at[rest], wd_ref.at[rest])

    def remote(src, dst, send, recv, device):
        return pltpu.make_async_remote_copy(
            src_ref=src, dst_ref=dst, send_sem=send, recv_sem=recv,
            device_id=device, device_id_type=MESH_ID,
        )

    def chunk_cols(c):
        if isinstance(c, int):
            return slice(c * cw, (c + 1) * cw)
        return pl.ds(pl.multiple_of(c * cw, cw), cw)

    cut = recv_part.shape[3]
    halves = (slice(0, cut), slice(cut, span))

    def rs_copy(c, tensor, n):
        s = (lax.rem(c, 2) * 3 + tensor) * 6 + n
        side_of = n % 2
        near, far = (beside, across) if side_of == 0 else (across, beside)
        rows = halves[side_of]
        size = rows.stop - rows.start
        owner = corner if n < 2 else near
        target = near if n < 4 else far
        if n < 4:
            src = send_part.at[c, tensor, owner, rows]
        else:
            src = pair_part.at[c, tensor, side_of, 0:size]
        return remote(
            src, recv_part.at[c, tensor, n, 0:size], rs_send.at[n], rs_recv.at[s], {"fs": target}
        )

    def product(c, tensor):
        cols = chunk_cols(c)
        if tensor == 0:
            value = jnp.dot(x_ref[...], wg_ref[:, cols], preferred_element_type=f32)
        elif tensor == 1:
            value = jnp.dot(x_ref[...], wu_ref[:, cols], preferred_element_type=f32)
        else:
            value = contract(og_ref[...], wd_ref[cols, :], 1, 1)
        value = value.astype(bf16)
        for g in range(n_fs):
            row = (g // 2) * (own_rows - HALO)
            lane = (g % 2) * LANES
            send_part[c, tensor, g] = value[row : row + span, lane : lane + LANES]

    def reduce_send(c, tensor):
        for n in range(4):
            rs_copy(c, tensor, n).start()

    def reduce_start(c, tensor):
        product(c, tensor)
        reduce_send(c, tensor)

    def combine(c, tensor):
        for n in range(2):
            rows = halves[n]
            size = rows.stop - rows.start
            rs_copy(c, tensor, n).wait_recv()
            mine = send_part[c, tensor, across if n == 0 else beside, rows]
            pair_part[c, tensor, n, 0:size] = (
                mine.astype(f32) + recv_part[c, tensor, n, 0:size].astype(f32)
            ).astype(bf16)
            rs_copy(c, tensor, 4 + n).start()

    def reduced(c, tensor):
        parts = []
        for n in range(2):
            rows = halves[n]
            size = rows.stop - rows.start
            rs_copy(c, tensor, 2 + n).wait_recv()
            value = send_part[c, tensor, f, rows].astype(f32) + recv_part[c, tensor, 2 + n, 0:size].astype(f32)
            rs_copy(c, tensor, 4 + n).wait_recv()
            parts.append(value + recv_part[c, tensor, 4 + n, 0:size].astype(f32))
        return jnp.concatenate(parts, axis=0).astype(bf16).astype(f32)

    def block(c, tensor, owner, part_of=None):
        col = lax.rem(owner, 2) * LANES
        row = (owner // 2) * own_rows
        if tensor == 0:
            size = LANES if part_of is None else LANES // 2
            start = col + (0 if part_of is None else part_of * size)
            return h_all.at[
                c, pl.ds(pl.multiple_of(start, size), size), pl.ds(pl.multiple_of(row, own_rows), own_rows)
            ]
        size = own_rows if part_of is None else own_rows // 2
        start = row + (0 if part_of is None else part_of * size)
        ref = g_all if tensor == 1 else u_all
        return ref.at[c, pl.ds(pl.multiple_of(start, size), size), pl.ds(pl.multiple_of(col, LANES), LANES)]

    def ag_copy(c, tensor, step, owner):
        s = (lax.rem(c, 2) * 3 + tensor) * 4
        if step == 0:
            ref, slot, target = block(c, tensor, owner), 0, beside
        elif step == 1:
            ref, slot, target = block(c, tensor, owner), 1, across
        elif step == 2:
            ref, slot, target = block(c, tensor, owner, 1), 2, beside
        else:
            ref, slot, target = block(c, tensor, owner, 0), 3, across
        return remote(ref, ref, ag_send.at[slot], ag_recv.at[s + slot], {"fs": target})

    def direct(c, tensor):
        return isinstance(c, int) and c == 0 and tensor < 2

    def corner_copy(c, tensor, owner):
        ref = block(c, tensor, owner)
        return remote(ref, ref, ag_send.at[4], ag_recv.at[tensor * 4 + 2], {"fs": corner})

    def gather_start(c, tensor):
        for step in (0, 1):
            ag_copy(c, tensor, step, f).start()
        if direct(c, tensor):
            corner_copy(c, tensor, f).start()

    def forward(c, tensor):
        ag_copy(c, tensor, 0, beside).wait_recv()
        ag_copy(c, tensor, 3, beside).start()
        ag_copy(c, tensor, 1, across).wait_recv()
        ag_copy(c, tensor, 2, across).start()

    def gathered(c, tensor, q):
        if direct(c, tensor):
            if q == 0:
                ag_copy(c, tensor, 1, across).wait_recv()
            if q == tensor ^ 1:
                ag_copy(c, tensor, 0, beside).wait_recv()
                corner_copy(c, tensor, corner).wait_recv()
        elif q == (1 if tensor == 0 else 0):
            ag_copy(c, tensor, 2, corner).wait_recv()
            ag_copy(c, tensor, 3, corner).wait_recv()

    def hidden_side(q):
        return side if q == 0 else 1 - side

    def own(value):
        return jnp.where(top == 0, value[:own_rows], value[HALO:])

    row_ids = lax.broadcasted_iota(jnp.int32, (span, LANES), 0)

    def down(value, lag):
        if lag == 0:
            return value
        return jnp.where(row_ids >= lag, pltpu.roll(value, lag, 0), 0.0)

    def up(value, lag):
        if lag == 0:
            return value
        return jnp.where(row_ids < span - lag, pltpu.roll(value, span - lag, 0), 0.0)

    def own_weights(c):
        cols = pl.ds(pl.multiple_of(c * cw + side * LANES, LANES), LANES)
        return taps_ref[:, cols].astype(f32)

    def hidden_step(c):
        weights = own_weights(c)
        gate = reduced(c, 0)
        pre = weights[0:1] * down(gate, KW - 1)
        for j in range(1, KW):
            pre = pre + weights[j : j + 1] * down(gate, KW - 1 - j)
        sig = 1.0 / (1.0 + jnp.exp(-pre))
        up_val = reduced(c, 1)
        h_all[c, own_cols, own_toks] = own(pre * sig * up_val).T.astype(bf16)
        gather_start(c, 0)
        held[0] = gate
        held[1] = up_val
        held[2] = pre
        held[3] = sig

    def grads_step(c):
        weights = own_weights(c)
        gate, up_val, pre, sig = held[0], held[1], held[2], held[3]
        act = reduced(c, 2)
        pre_grad = act * up_val * sig * (1.0 + pre * (1.0 - sig))
        grad = weights[0:1] * up(pre_grad, KW - 1)
        for j in range(1, KW):
            grad = grad + weights[j : j + 1] * up(pre_grad, KW - 1 - j)
        g_all[c, own_toks, own_cols] = own(grad).astype(bf16)
        u_all[c, own_toks, own_cols] = own(act * (pre * sig)).astype(bf16)
        for j in range(KW):
            tap_all[f, pl.ds(c * KW + j, 1), :] = jnp.sum(
                own(down(gate, KW - 1 - j) * pre_grad), axis=0, keepdims=True
            )

    def half_rows(h):
        return slice(h * LANES, (h + 1) * LANES)

    def part_copy(p, h):
        rows = half_rows(h)
        s = lax.rem(p * per + h, KEEP)
        return remote(part.at[p, rows], from_out.at[p, rows], a_send.at[0], out_recv.at[s], {"rep": toward})

    def exchange_copy(p, h):
        rows = half_rows(h)
        s = lax.rem(p * per + h, KEEP)
        return remote(part.at[p, rows], from_in.at[p, rows], a_send.at[0], in_recv.at[s], {"rep": toward})

    def total_copy(p, h):
        rows = half_rows(h)
        s = lax.rem(p * per + h, KEEP)
        return remote(tot.at[p, rows], from_in.at[p, rows], b_send.at[0], in_recv.at[s], {"rep": outward})

    def piece_rows(base, h):
        if isinstance(base, int) and isinstance(h, int):
            return slice(base + h * LANES, base + (h + 1) * LANES)
        return pl.ds(pl.multiple_of(base + h * LANES, LANES), LANES)

    def place(c, s, h):
        tensor, q = s // subs, s % subs
        slot = (s * per + h) % WIDE
        if tensor == 0:
            dst = down_ref.at[piece_rows(c * cw, hidden_side(q)), h * cw : (h + 1) * cw]
        elif tensor == 1:
            dst = gate_ref.at[piece_rows(q * cw, h), chunk_cols(c)]
        else:
            dst = up_ref.at[piece_rows(q * cw, h), chunk_cols(c)]
        return pltpu.make_async_copy(wide.at[slot], dst, wide_sem.at[slot])

    def finished(c, s, h, value):
        tensor, q = s // subs, s % subs
        value = value.astype(f32)
        slot = (s * per + h) % WIDE
        copy = place(c, s, h)
        if not isinstance(c, int):
            pl.when((c * slots + s) * per + h >= WIDE)(copy.wait)
        elif (c * slots + s) * per + h >= WIDE:
            copy.wait()
        wide[slot] = value
        copy.start()
        square = value * value
        lanes = square[:, :LANES]
        for g in range(1, cw // LANES):
            lanes = lanes + square[:, g * LANES : (g + 1) * LANES]
        row = jnp.sum(lanes.T, axis=0, keepdims=True)
        if tensor == 0:
            at = pl.ds(c * per + hidden_side(q), 1)
            rows_d[at, :] = row if h == 0 else rows_d[at, :] + row
        else:
            at = ((tensor - 1) * subs + q) * per + h
            rows_gu[at : at + 1, :] = rows_gu[at : at + 1, :] + row

    def stage_a(p, h):
        part_copy(p, h).wait_recv()
        rows = half_rows(h)
        part[p, rows] = (ring[lax.rem(p, RING), rows] + from_out[p, rows].astype(f32)).astype(bf16)
        exchange_copy(p, h).start()

    def stage_b(c, s, h):
        p = c * slots + s
        rows = half_rows(h)
        exchange_copy(p, h).wait_recv()
        value = (part[p, rows].astype(f32) + from_in[p, rows].astype(f32)).astype(bf16)
        tot[p, rows] = value
        total_copy(p, h).start()
        finished(c, s, h, value)

    def stage_out(c, s, h):
        p = c * slots + s
        exchange_copy(p, h).wait_recv()
        finished(c, s, h, from_in[p, half_rows(h)])

    def behind(c, s, h, lag):
        steps = slots * per
        at = s * per + h - lag
        back = (-at + steps - 1) // steps if at < 0 else 0
        at += back * steps
        return c - back, at // per, at % per, back

    def guarded(c, lowest, fn):
        if isinstance(c, int):
            if c >= lowest:
                fn()
        elif lowest <= 1:
            fn()
        else:
            pl.when(c >= lowest)(fn)

    def work(c, s):
        tensor, q = s // subs, s % subs
        p = c * slots + s

        def middle(h):
            ca, sa, ha, ka = behind(c, s, h, A_LAG)
            guarded(c, ka, functools.partial(stage_a, ca * slots + sa, ha))
            cb, sb, hb, kb = behind(c, s, h, B_LAG)
            guarded(c, kb, functools.partial(stage_b, cb, sb, hb))

        if not isinstance(c, int) or c > 0 or s > 0:
            pl.when(is_mid)(lambda: middle(0))
        gathered(c, tensor, q)
        if tensor == 0:
            rows = pl.ds(pl.multiple_of(hidden_side(q) * LANES, LANES), LANES)
            value = jnp.dot(h_all[c, rows, :], og_ref[...], preferred_element_type=f32)
            value = jnp.concatenate([value[:, n * cw : (n + 1) * cw] for n in range(subs)], axis=0)
        elif tensor == 1:
            value = jnp.dot(xt[q], g_all[c], preferred_element_type=f32)
        else:
            value = jnp.dot(xt[q], u_all[c], preferred_element_type=f32)

        @pl.when(is_end)
        def _():
            for h in range(per):
                part[p, half_rows(h)] = value[half_rows(h)].astype(bf16)
                part_copy(p, h).start()
            for h in range(per):
                co, so, ho, ko = behind(c, s, h, OUT_LAG)
                guarded(c, ko, functools.partial(stage_out, co, so, ho))

        @pl.when(is_mid)
        def _():
            ring[lax.rem(p, RING)] = value
            middle(1)

    def input_term(c):
        cols = chunk_cols(c)
        term = contract(g_all[c], wg_ref[:, cols], 1, 1) + contract(u_all[c], wu_ref[:, cols], 1, 1)
        if isinstance(c, int) and c == 0:
            acc[...] = term
        else:
            acc[...] += term

    actions = {
        "forward": forward,
        "reduce": reduce_start,
        "combine": combine,
        "hidden": lambda c, tensor: hidden_step(c),
        "grads": lambda c, tensor: grads_step(c),
        "gather": gather_start,
    }

    def run(step, c):
        name, ahead, tensor = step
        target = c + ahead
        if isinstance(c, int):
            if target < chunks:
                actions[name](target, tensor)
        elif ahead == 0:
            actions[name](target, tensor)
        else:
            pl.when(target < chunks)(lambda: actions[name](target, tensor))

    m = 2 * (n_fs - 1)
    half = tok // 2
    ig_copy = remote(
        ig_send.at[pl.ds(pl.multiple_of((1 - t) * half, half), half)], ig_recv,
        misc.at[m], misc.at[m + 1], {"tp": 1 - t},
    )
    tap_peers = [
        remote(tap_all.at[f], tap_all.at[f], misc.at[2 * k], misc.at[2 * k + 1], {"fs": peers[k]})
        for k in range(n_fs - 1)
    ]
    tap_part = remote(tap_two, tap_out, misc.at[m + 2], misc.at[m + 3], {"rep": toward})
    tap_exchange = remote(tap_two, tap_in, misc.at[m + 2], misc.at[m + 4], {"rep": toward})
    tap_total = remote(tap_sum, tap_in, misc.at[m + 5], misc.at[m + 4], {"rep": outward})
    fs_rows = [
        remote(rows_d, rows_fs.at[k], misc.at[m + 8 + 2 * k], misc.at[m + 9 + 2 * k], {"fs": peers[k]})
        for k in range(n_fs - 1)
    ]
    tp_rows = remote(rows_gu, rows_tp, misc.at[m + 6], misc.at[m + 7], {"tp": 1 - t})

    outputs = [
        pltpu.make_async_copy(src, dst, out_sem.at[n])
        for n, (src, dst) in enumerate((
            (in_grad_ref, in_grad_out), (taps_out_ref, taps_out),
            (rows_down_ref, rows_down_out), (rows_gu_ref, rows_gu_out),
        ))
    ]

    def tap_first():
        for copy in tap_peers:
            copy.wait()
        for i in range(per):
            tap_two[i] = tap_all[i] + tap_all[i + 2]
        pl.when(is_end)(tap_part.start)

    def tap_second():
        tap_part.wait_recv()
        tap_two[...] = tap_two[...] + tap_out[...]
        tap_exchange.start()

    def tap_place():
        for c in range(chunks):
            for i in range(per):
                lane = (c * per + i) * LANES
                taps_out_ref[:, lane : lane + LANES] = tap_sum[i, c * KW : (c + 1) * KW, :]
        outputs[1].start()

    def input_start():
        ig_send[...] = acc[...].astype(bf16)
        ig_copy.start()

    def input_finish():
        ig_copy.wait()
        in_grad_ref[...] = (
            ig_send[pl.ds(pl.multiple_of(t * half, half), half), :].astype(f32) + ig_recv[...].astype(f32)
        ).astype(bf16)
        outputs[0].start()

    def body(c, last=False):
        for s in range(slots):
            for step in (FIRST_STEPS if isinstance(c, int) and c == 0 else STEPS)[s]:
                run(step, c)
            if last and s == 1:
                for copy in tap_peers:
                    copy.start()
            if last and s == 3:
                tap_first()
            if last and s == slots - 2:
                pl.when(is_mid)(tap_second)
            work(c, s)
        input_term(c)

    loads[0].wait()
    loads[1].wait()
    product(0, 0)
    loads[2].wait()
    product(0, 1)
    pl.semaphore_wait(barrier, n_fs + 1 + jnp.where(is_mid, 1, 0))
    pl.when(t == 1)(lambda: pl.semaphore_wait(go_sem, 1))
    reduce_send(0, 0)
    reduce_send(0, 1)
    loads[3].wait()
    loads[4].wait()
    reduce_start(0, 2)
    for q in range(subs):
        xt[q] = x_ref[:, q * cw : (q + 1) * cw].astype(f32).T.astype(bf16)
    rows_gu[...] = jnp.zeros_like(rows_gu)
    for copy in loads[5:]:
        copy.wait()
    combine(0, 0)

    @pl.when(t == 0)
    def _():
        pl.semaphore_signal(go_sem, inc=1, device_id={"tp": 1 - t}, device_id_type=MESH_ID)

    combine(0, 1)
    product(1, 0)
    combine(0, 2)
    hidden_step(0)
    grads_step(0)
    gather_start(0, 1)
    reduce_send(1, 0)
    reduce_start(1, 1)
    body(0)

    @pl.loop(1, chunks - 1)
    def _(c):
        body(c)

    body(chunks - 1, last=True)
    input_start()
    down_last = total_pieces - slots + subs - 1

    steps = total_pieces * per

    @pl.when(is_end)
    def _():
        for k in range(steps - OUT_LAG, steps):
            p = k // per
            if k == steps - 1:
                input_finish()
                tap_exchange.wait_recv()
                tap_sum[...] = tap_in[...]
                tap_place()
            stage_out(p // slots, p % slots, k % per)
            if k == max(steps - OUT_LAG, (down_last + 1) * per - 1):
                for copy in fs_rows:
                    copy.start()

    @pl.when(is_mid)
    def _():
        for copy in fs_rows:
            copy.start()
        for k in range(steps, steps + B_LAG):
            if k - A_LAG < steps:
                stage_a((k - A_LAG) // per, (k - A_LAG) % per)
            p = (k - B_LAG) // per
            stage_b(p // slots, p % slots, (k - B_LAG) % per)
            if k == steps:
                tap_exchange.wait_recv()
                tap_sum[...] = tap_two[...] + tap_in[...]
                tap_total.start()
                input_finish()
                tap_place()

    tp_rows.start()

    def all_sent(ref, sem):
        remote(ref, ref, sem, sem, {"tp": 1 - t}).wait_send()

    for n in range(6):
        rows = halves[n % 2]
        all_sent(recv_part.at[:, :, n, 0 : rows.stop - rows.start], rs_send.at[n])
    blocks = chunks * 3
    for slot in range(2):
        all_sent(part.at[0:blocks, 0 : own_rows // 2], ag_send.at[slot])
    for slot in range(2, 4):
        all_sent(part.at[0 : blocks - 2, 0 : own_rows // 4], ag_send.at[slot])
    all_sent(part.at[0:2, 0 : own_rows // 2], ag_send.at[4])
    all_sent(part, a_send.at[0])
    tap_part.wait_send()

    @pl.when(is_mid)
    def _():
        all_sent(tot, b_send.at[0])

    for k in range(steps - WIDE, steps):
        p = k // per
        place(p // slots, p % slots, k % per).wait()
    for copy in fs_rows:
        copy.wait()
    rows_down_ref[...] = rows_d[...] + (rows_fs[0] + rows_fs[1] + rows_fs[2])
    outputs[2].start()
    tp_rows.wait()
    rows_gu_ref[...] = rows_gu[...] + rows_tp[...]
    outputs[3].start()
    for copy in outputs:
        copy.wait()

    @pl.when(is_mid)
    def _():
        tap_total.wait_send()


def finish_kernel(
    gate, up, down, in_grad, taps, rows_gu, rows_d,
    gate_out, up_out, down_out, in_grad_out, taps_out, rows_gate_out, rows_up_out, rows_down_out,
    rows_gate, rows_up, rows_down, sems,
):
    copies = []

    def send(src, dst):
        copy = pltpu.make_async_copy(src, dst, sems.at[len(copies)])
        copy.start()
        copies.append(copy)

    for src, dst in ((gate, gate_out), (up, up_out), (down, down_out), (in_grad, in_grad_out), (taps, taps_out)):
        send(src, dst)
    groups = rows_gate.shape[0] // LANES
    for i in range(groups):
        rows_gate[pl.ds(i * LANES, LANES)] = rows_gu[i]
        rows_up[pl.ds(i * LANES, LANES)] = rows_gu[groups + i]
    for i in range(rows_down.shape[0] // LANES):
        rows_down[pl.ds(i * LANES, LANES)] = rows_d[i]
    for src, dst in ((rows_gate, rows_gate_out), (rows_up, rows_up_out), (rows_down, rows_down_out)):
        send(src, dst)
    for copy in copies:
        copy.wait()


def fits(shape, inputs, w_gate):
    n_rep, n_fs, n_tp = shape["rep"], shape["fs"], shape["tp"]
    tok, feat = inputs.shape
    return (
        n_rep == 4 and n_fs == 4 and n_tp == 2 and feat == 2 * CW and 3 * CW <= w_gate.shape[1]
        and w_gate.shape[1] % CW == 0 and w_gate.shape[1] <= 1536 and tok % (2 * LANES) == 0 and tok <= 512
    )


def fused_shards(shape, inputs, w_gate, w_up, conv_taps, w_down, out_grad):
    if not fits(shape, inputs, w_gate):
        return shards(inputs, w_gate, w_up, conv_taps, w_down, out_grad)
    n_rep, n_fs = shape["rep"], shape["fs"]
    tok, feat = inputs.shape
    hid = w_gate.shape[1]
    cw = CW
    chunks = hid // cw
    subs = feat // cw
    per = cw // LANES
    pieces = chunks * 3 * subs
    span = tok // 2 + HALO
    cut = -(-span // (2 * HALO)) * HALO
    bf16, f32 = jnp.bfloat16, jnp.float32
    vmem = pl.BlockSpec(memory_space=pltpu.VMEM)
    hbm = pl.BlockSpec(memory_space=pltpu.HBM)
    anywhere = pl.BlockSpec(memory_space=pl.ANY)
    dma = pltpu.SemaphoreType.DMA
    local = pltpu.VMEM
    whole = jax.ShapeDtypeStruct
    in_grad, down, gate, up, taps, rows_gu, rows_d = pl.pallas_call(
        functools.partial(layer_kernel, n_rep, n_fs),
        out_shape=(
            local((tok // 2, feat), bf16),
            local((hid, feat), f32),
            local((feat, hid), f32),
            local((feat, hid), f32),
            local((KW, hid), f32),
            local((2 * subs * per, LANES), f32),
            local((chunks * per, LANES), f32),
        ),
        in_specs=[hbm, hbm, hbm, vmem, hbm, hbm],
        out_specs=(anywhere,) * 7,
        scratch_shapes=[
            local((tok, feat), bf16),
            local((feat, hid), bf16),
            local((feat, hid), bf16),
            local((hid, feat), bf16),
            local((tok, feat), bf16),
            local((subs, cw, tok), bf16),
            local((chunks, 3, n_fs, span, LANES), bf16),
            local((chunks, 3, 6, cut, LANES), bf16),
            local((chunks, 3, 2, cut, LANES), bf16),
            local((4, span, LANES), f32),
            local((chunks, cw, tok), bf16),
            local((chunks, tok, cw), bf16),
            local((chunks, tok, cw), bf16),
            local((RING, cw, cw), f32),
            local((WIDE, LANES, cw), f32),
            local((pieces, cw, cw), bf16),
            local((pieces, cw, cw), bf16),
            local((pieces, cw, cw), bf16),
            local((pieces, cw, cw), bf16),
            local((tok, feat), f32),
            local((tok, feat), bf16),
            local((tok // 2, feat), bf16),
            local((tok // 2, feat), bf16),
            local((KW, hid), f32),
            local((2 * subs * per, LANES), f32),
            local((chunks * per, LANES), f32),
            local((n_fs, chunks * KW, LANES), f32),
            local((per, chunks * KW, LANES), f32),
            local((per, chunks * KW, LANES), f32),
            local((per, chunks * KW, LANES), f32),
            local((per, chunks * KW, LANES), f32),
            local((2 * subs * per, LANES), f32),
            local((chunks * per, LANES), f32),
            local((2 * subs * per, LANES), f32),
            local((n_fs - 1, chunks * per, LANES), f32),
            dma((6,)), dma((36,)), dma((5,)), dma((24,)),
            dma((1,)), dma((KEEP,)), dma((KEEP,)), dma((1,)), dma((WIDE,)), dma((4,)), dma((8,)), pltpu.SemaphoreType.REGULAR,
            dma((4 * (n_fs - 1) + 8,)),
        ],
        compiler_params=pltpu.CompilerParams(
            collective_id=0, has_side_effects=True, vmem_limit_bytes=50 * 1024 * 1024
        ),
    )(inputs, w_gate, w_up, conv_taps, w_down, out_grad)
    gate, up, down, in_grad, taps, rows_gate, rows_up, rows_down = pl.pallas_call(
        finish_kernel,
        out_shape=(
            whole((feat, hid), f32), whole((feat, hid), f32), whole((hid, feat), f32),
            whole((tok // 2, feat), bf16), whole((KW, hid), f32),
            whole((feat,), f32), whole((feat,), f32), whole((hid,), f32),
        ),
        in_specs=[anywhere] * 5 + [vmem] * 2,
        out_specs=(anywhere,) * 8,
        scratch_shapes=[local((feat,), f32), local((feat,), f32), local((hid,), f32), dma((8,))],
        compiler_params=pltpu.CompilerParams(vmem_limit_bytes=24 * 1024 * 1024),
    )(gate, up, down, in_grad, taps, rows_gu, rows_d)
    return (in_grad, gate, up, down, taps, rows_gate, rows_up, rows_down)


def solution(mesh):
    return jax.shard_map(
        functools.partial(fused_shards, dict(mesh.shape)),
        mesh=mesh,
        in_specs=(
            P("rep", "fs"),
            P("fs", "tp"),
            P("fs", "tp"),
            P(None, "tp"),
            P("tp", "fs"),
            P("rep", "fs"),
        ),
        out_specs=(
            P(("rep", "tp"), "fs"),
            P("fs", "tp"),
            P("fs", "tp"),
            P("tp", "fs"),
            P(None, "tp"),
            P("fs"),
            P("fs"),
            P("tp"),
        ),
        check_vma=False,
    )
```

```python
import functools

import jax
import jax.numpy as jnp
from jax import lax
from jax.experimental import pallas as pl
from jax.experimental.pallas import tpu as pltpu
from jax.sharding import PartitionSpec as P

KW = 3


def shift_down(values, lag_rows):
    if lag_rows == 0:
        return values
    padding = jnp.zeros_like(values[:lag_rows])
    return jnp.concatenate([padding, values[:-lag_rows]], axis=0)


def shift_up(values, lag_rows):
    if lag_rows == 0:
        return values
    padding = jnp.zeros_like(values[:lag_rows])
    return jnp.concatenate([values[lag_rows:], padding], axis=0)


def contract(left, right, left_dim, right_dim):
    return lax.dot_general(
        left, right, (((left_dim,), (right_dim,)), ((), ())), preferred_element_type=jnp.float32
    )


def row_norms(grad_gate, grad_up, grad_down):
    gate_rows = jnp.sum(grad_gate * grad_gate, axis=1)
    up_rows = jnp.sum(grad_up * grad_up, axis=1)
    down_rows = jnp.sum(grad_down * grad_down, axis=1)
    gate_rows, up_rows = lax.psum((gate_rows, up_rows), "tp")
    down_rows = lax.psum(down_rows, "fs")
    return (gate_rows, up_rows, down_rows)


def shards(inputs, w_gate, w_up, conv_taps, w_down, out_grad):
    tap_weights = conv_taps.astype(jnp.float32)
    gate_part = jnp.dot(inputs, w_gate, preferred_element_type=jnp.float32)
    up_part = jnp.dot(inputs, w_up, preferred_element_type=jnp.float32)
    act_part = contract(out_grad, w_down, 1, 1)
    gate_sum, up_sum, act_sum = (
        lax.psum(gate_part.astype(jnp.bfloat16), "fs").astype(jnp.float32),
        lax.psum(up_part.astype(jnp.bfloat16), "fs").astype(jnp.float32),
        lax.psum(act_part.astype(jnp.bfloat16), "fs").astype(jnp.float32),
    )
    gate_pre = gate_sum.astype(jnp.bfloat16)
    up_val = up_sum.astype(jnp.bfloat16)
    act_grad = act_sum.astype(jnp.bfloat16)
    gate_float = gate_pre.astype(jnp.float32)
    up_float = up_val.astype(jnp.float32)
    act_float = act_grad.astype(jnp.float32)
    shifted = [shift_down(gate_float, KW - 1 - tap_index) for tap_index in range(KW)]
    pre_act = tap_weights[0] * shifted[0]
    for tap_index in range(1, KW):
        pre_act = pre_act + tap_weights[tap_index] * shifted[tap_index]
    sigmoid_pre = jax.nn.sigmoid(pre_act)
    hidden = (pre_act * sigmoid_pre * up_float).astype(jnp.bfloat16)
    up_grad = (act_float * pre_act * sigmoid_pre).astype(jnp.bfloat16)
    pre_grad = act_float * up_float * sigmoid_pre * (1.0 + pre_act * (1.0 - sigmoid_pre))
    gate_acc = tap_weights[0] * shift_up(pre_grad, KW - 1)
    for tap_index in range(1, KW):
        gate_acc = gate_acc + tap_weights[tap_index] * shift_up(pre_grad, KW - 1 - tap_index)
    gate_grad = gate_acc.astype(jnp.bfloat16)
    gate_rows = gate_grad
    up_rows = up_grad
    in_grad = lax.psum_scatter(
        (contract(gate_rows, w_gate, 1, 1) + contract(up_rows, w_up, 1, 1)).astype(jnp.bfloat16),
        "tp",
        scatter_dimension=0,
        tiled=True,
    )
    grad_gate = contract(inputs, gate_grad, 0, 0)
    grad_up = contract(inputs, up_grad, 0, 0)
    grad_down = contract(hidden, out_grad, 0, 0)
    grad_taps = jnp.stack(
        [jnp.sum(shifted[tap_index] * pre_grad, axis=0) for tap_index in range(KW)]
    )
    grad_gate, grad_up, grad_down, grad_taps = (
        lax.psum(grad_gate.astype(jnp.bfloat16), "rep").astype(jnp.float32),
        lax.psum(grad_up.astype(jnp.bfloat16), "rep").astype(jnp.float32),
        lax.psum(grad_down.astype(jnp.bfloat16), "rep").astype(jnp.float32),
        lax.psum(grad_taps.astype(jnp.bfloat16), "rep").astype(jnp.float32),
    )
    gate_rows, up_rows, down_rows = row_norms(grad_gate, grad_up, grad_down)
    weight_grads = (grad_gate, grad_up, grad_down, grad_taps, gate_rows, up_rows, down_rows)
    grad_gate, grad_up, grad_down, grad_taps, gate_rows, up_rows, down_rows = weight_grads
    return (in_grad, grad_gate, grad_up, grad_down, grad_taps, gate_rows, up_rows, down_rows)


LANES = 128
CW = 256
HALO = 16
A_LAG = 1
B_LAG = 4
OUT_LAG = 18
RING = 2
WIDE = 4
KEEP = 24
MESH_ID = pl.DeviceIdType.MESH

STEPS = (
    (("grads", 0, 0), ("gather", 0, 1), ("reduce", 1, 0)),
    (("forward", 0, 1), ("gather", 0, 2)),
    (("combine", 1, 0), ("combine", 1, 1), ("reduce", 1, 2)),
    (("forward", 0, 2),),
    (("hidden", 1, 0), ("combine", 1, 2), ("reduce", 2, 1)),
    (("forward", 1, 0),),
)
FIRST_STEPS = ((), (("gather", 0, 2),), (), STEPS[2] + STEPS[3]) + STEPS[4:]


def layer_kernel(
    n_rep, n_fs,
    x_hbm, wg_hbm, wu_hbm, taps_hbm, wd_hbm, og_hbm,
    in_grad_out, down_ref, gate_ref, up_ref, taps_out, rows_gu_out, rows_down_out,
    x_ref, wg_ref, wu_ref, taps_ref, wd_ref, og_ref,
    xt, send_part, recv_part, pair_part, held, h_all, g_all, u_all, ring, wide, part, from_out, from_in, tot,
    acc, ig_send, ig_recv, in_grad_ref, taps_out_ref, rows_gu_ref, rows_down_ref, tap_all, tap_two, tap_out, tap_in, tap_sum, rows_gu, rows_d, rows_tp, rows_fs,
    rs_send, rs_recv, ag_send, ag_recv, a_send, out_recv, in_recv, b_send, wide_sem, out_sem, loc_sem, go_sem, misc,
):
    tok, feat = x_ref.shape
    cw = CW
    chunks = wg_ref.shape[1] // cw
    subs = feat // cw
    own_rows = tok // 2
    span = own_rows + HALO
    slots = 3 * subs
    total_pieces = chunks * slots
    per = cw // LANES
    f32, bf16 = jnp.float32, jnp.bfloat16
    r = lax.axis_index("rep")
    f = lax.axis_index("fs")
    t = lax.axis_index("tp")
    half_rep = n_rep // 2
    is_left = r < half_rep
    toward = jnp.where(is_left, r + 1, r - 1)
    outward = jnp.where(is_left, r - 1, r + 1)
    is_end = jnp.logical_or(r == 0, r == n_rep - 1)
    is_mid = jnp.logical_not(is_end)
    beside = f + 1 - 2 * lax.rem(f, 2)
    across = lax.rem(f + 2, 4)
    corner = lax.rem(beside + 2, 4)
    peers = [beside, across, corner]
    side = lax.rem(f, 2)
    top = f // 2
    own_cols = pl.ds(pl.multiple_of(side * LANES, LANES), LANES)
    own_toks = pl.ds(pl.multiple_of(top * own_rows, own_rows), own_rows)

    barrier = pltpu.get_barrier_semaphore()
    for k in range(n_fs - 1):
        pl.semaphore_signal(barrier, inc=1, device_id={"fs": peers[k]}, device_id_type=MESH_ID)
    pl.semaphore_signal(barrier, inc=1, device_id={"tp": 1 - t}, device_id_type=MESH_ID)
    pl.semaphore_signal(barrier, inc=1, device_id={"rep": toward}, device_id_type=MESH_ID)

    @pl.when(is_mid)
    def _():
        pl.semaphore_signal(barrier, inc=1, device_id={"rep": outward}, device_id_type=MESH_ID)

    loads = []

    def load(src, dst):
        copy = pltpu.make_async_copy(src, dst, loc_sem.at[len(loads)])
        copy.start()
        loads.append(copy)

    first = slice(0, cw)
    load(x_hbm, x_ref)
    load(wg_hbm.at[:, first], wg_ref.at[:, first])
    load(wu_hbm.at[:, first], wu_ref.at[:, first])
    load(og_hbm, og_ref)
    load(wd_hbm.at[first], wd_ref.at[first])
    load(taps_hbm, taps_ref)
    if chunks > 1:
        rest = slice(cw, chunks * cw)
        load(wg_hbm.at[:, rest], wg_ref.at[:, rest])
        load(wu_hbm.at[:, rest], wu_ref.at[:, rest])
        load(wd_hbm.at[rest], wd_ref.at[rest])

    def remote(src, dst, send, recv, device):
        return pltpu.make_async_remote_copy(
            src_ref=src, dst_ref=dst, send_sem=send, recv_sem=recv,
            device_id=device, device_id_type=MESH_ID,
        )

    def chunk_cols(c):
        if isinstance(c, int):
            return slice(c * cw, (c + 1) * cw)
        return pl.ds(pl.multiple_of(c * cw, cw), cw)

    cut = recv_part.shape[3]
    halves = (slice(0, cut), slice(cut, span))

    def rs_copy(c, tensor, n):
        s = (lax.rem(c, 2) * 3 + tensor) * 6 + n
        side_of = n % 2
        near, far = (beside, across) if side_of == 0 else (across, beside)
        rows = halves[side_of]
        size = rows.stop - rows.start
        owner = corner if n < 2 else near
        target = near if n < 4 else far
        if n < 4:
            src = send_part.at[c, tensor, owner, rows]
        else:
            src = pair_part.at[c, tensor, side_of, 0:size]
        return remote(
            src, recv_part.at[c, tensor, n, 0:size], rs_send.at[n], rs_recv.at[s], {"fs": target}
        )

    def product(c, tensor):
        cols = chunk_cols(c)
        if tensor == 0:
            value = jnp.dot(x_ref[...], wg_ref[:, cols], preferred_element_type=f32)
        elif tensor == 1:
            value = jnp.dot(x_ref[...], wu_ref[:, cols], preferred_element_type=f32)
        else:
            value = contract(og_ref[...], wd_ref[cols, :], 1, 1)
        value = value.astype(bf16)
        for g in range(n_fs):
            row = (g // 2) * (own_rows - HALO)
            lane = (g % 2) * LANES
            send_part[c, tensor, g] = value[row : row + span, lane : lane + LANES]

    def reduce_send(c, tensor, steps=range(4)):
        for n in steps:
            rs_copy(c, tensor, n).start()

    def reduce_start(c, tensor):
        product(c, tensor)
        reduce_send(c, tensor)

    def combine(c, tensor):
        for n in range(2):
            rows = halves[n]
            size = rows.stop - rows.start
            rs_copy(c, tensor, n).wait_recv()
            mine = send_part[c, tensor, across if n == 0 else beside, rows]
            pair_part[c, tensor, n, 0:size] = (
                mine.astype(f32) + recv_part[c, tensor, n, 0:size].astype(f32)
            ).astype(bf16)
            rs_copy(c, tensor, 4 + n).start()

    def reduced(c, tensor):
        parts = []
        for n in range(2):
            rows = halves[n]
            size = rows.stop - rows.start
            rs_copy(c, tensor, 2 + n).wait_recv()
            value = send_part[c, tensor, f, rows].astype(f32) + recv_part[c, tensor, 2 + n, 0:size].astype(f32)
            rs_copy(c, tensor, 4 + n).wait_recv()
            parts.append(value + recv_part[c, tensor, 4 + n, 0:size].astype(f32))
        return jnp.concatenate(parts, axis=0).astype(bf16).astype(f32)

    def block(c, tensor, owner, part_of=None):
        col = lax.rem(owner, 2) * LANES
        row = (owner // 2) * own_rows
        if tensor == 0:
            size = LANES if part_of is None else LANES // 2
            start = col + (0 if part_of is None else part_of * size)
            return h_all.at[
                c, pl.ds(pl.multiple_of(start, size), size), pl.ds(pl.multiple_of(row, own_rows), own_rows)
            ]
        size = own_rows if part_of is None else own_rows // 2
        start = row + (0 if part_of is None else part_of * size)
        ref = g_all if tensor == 1 else u_all
        return ref.at[c, pl.ds(pl.multiple_of(start, size), size), pl.ds(pl.multiple_of(col, LANES), LANES)]

    def ag_copy(c, tensor, step, owner):
        s = (lax.rem(c, 2) * 3 + tensor) * 4
        if step == 0:
            ref, slot, target = block(c, tensor, owner), 0, beside
        elif step == 1:
            ref, slot, target = block(c, tensor, owner), 1, across
        elif step == 2:
            ref, slot, target = block(c, tensor, owner, 1), 2, beside
        else:
            ref, slot, target = block(c, tensor, owner, 0), 3, across
        return remote(ref, ref, ag_send.at[slot], ag_recv.at[s + slot], {"fs": target})

    def direct(c, tensor):
        return isinstance(c, int) and c == 0 and tensor < 2

    def corner_copy(c, tensor, owner):
        ref = block(c, tensor, owner)
        return remote(ref, ref, ag_send.at[4], ag_recv.at[tensor * 4 + 2], {"fs": corner})

    def gather_start(c, tensor):
        for step in (0, 1):
            ag_copy(c, tensor, step, f).start()
        if direct(c, tensor):
            corner_copy(c, tensor, f).start()

    def forward(c, tensor):
        ag_copy(c, tensor, 0, beside).wait_recv()
        ag_copy(c, tensor, 3, beside).start()
        ag_copy(c, tensor, 1, across).wait_recv()
        ag_copy(c, tensor, 2, across).start()

    def gathered(c, tensor, q):
        if direct(c, tensor):
            if q == 0:
                ag_copy(c, tensor, 1, across).wait_recv()
            if q == tensor ^ 1:
                ag_copy(c, tensor, 0, beside).wait_recv()
                corner_copy(c, tensor, corner).wait_recv()
        elif q == (1 if tensor == 0 else 0):
            ag_copy(c, tensor, 2, corner).wait_recv()
            ag_copy(c, tensor, 3, corner).wait_recv()

    def hidden_side(q):
        return side if q == 0 else 1 - side

    def own(value):
        return jnp.where(top == 0, value[:own_rows], value[HALO:])

    row_ids = lax.broadcasted_iota(jnp.int32, (span, LANES), 0)

    def down(value, lag):
        if lag == 0:
            return value
        return jnp.where(row_ids >= lag, pltpu.roll(value, lag, 0), 0.0)

    def up(value, lag):
        if lag == 0:
            return value
        return jnp.where(row_ids < span - lag, pltpu.roll(value, span - lag, 0), 0.0)

    def own_weights(c):
        cols = pl.ds(pl.multiple_of(c * cw + side * LANES, LANES), LANES)
        return taps_ref[:, cols].astype(f32)

    def hidden_step(c):
        weights = own_weights(c)
        gate = reduced(c, 0)
        pre = weights[0:1] * down(gate, KW - 1)
        for j in range(1, KW):
            pre = pre + weights[j : j + 1] * down(gate, KW - 1 - j)
        sig = 1.0 / (1.0 + jnp.exp(-pre))
        up_val = reduced(c, 1)
        h_all[c, own_cols, own_toks] = own(pre * sig * up_val).T.astype(bf16)
        gather_start(c, 0)
        held[0] = gate
        held[1] = up_val
        held[2] = pre
        held[3] = sig

    def grads_step(c):
        weights = own_weights(c)
        gate, up_val, pre, sig = held[0], held[1], held[2], held[3]
        act = reduced(c, 2)
        pre_grad = act * up_val * sig * (1.0 + pre * (1.0 - sig))
        grad = weights[0:1] * up(pre_grad, KW - 1)
        for j in range(1, KW):
            grad = grad + weights[j : j + 1] * up(pre_grad, KW - 1 - j)
        g_all[c, own_toks, own_cols] = own(grad).astype(bf16)
        u_all[c, own_toks, own_cols] = own(act * (pre * sig)).astype(bf16)
        for j in range(KW):
            tap_all[f, pl.ds(c * KW + j, 1), :] = jnp.sum(
                own(down(gate, KW - 1 - j) * pre_grad), axis=0, keepdims=True
            )

    def half_rows(h):
        return slice(h * LANES, (h + 1) * LANES)

    def part_copy(p, h):
        rows = half_rows(h)
        s = lax.rem(p * per + h, KEEP)
        return remote(part.at[p, rows], from_out.at[p, rows], a_send.at[0], out_recv.at[s], {"rep": toward})

    def exchange_copy(p, h):
        rows = half_rows(h)
        s = lax.rem(p * per + h, KEEP)
        return remote(part.at[p, rows], from_in.at[p, rows], a_send.at[0], in_recv.at[s], {"rep": toward})

    def total_copy(p, h):
        rows = half_rows(h)
        s = lax.rem(p * per + h, KEEP)
        return remote(tot.at[p, rows], from_in.at[p, rows], b_send.at[0], in_recv.at[s], {"rep": outward})

    def piece_rows(base, h):
        if isinstance(base, int) and isinstance(h, int):
            return slice(base + h * LANES, base + (h + 1) * LANES)
        return pl.ds(pl.multiple_of(base + h * LANES, LANES), LANES)

    def place(c, s, h):
        tensor, q = s // subs, s % subs
        slot = (s * per + h) % WIDE
        if tensor == 0:
            dst = down_ref.at[piece_rows(c * cw, hidden_side(q)), h * cw : (h + 1) * cw]
        elif tensor == 1:
            dst = gate_ref.at[piece_rows(q * cw, h), chunk_cols(c)]
        else:
            dst = up_ref.at[piece_rows(q * cw, h), chunk_cols(c)]
        return pltpu.make_async_copy(wide.at[slot], dst, wide_sem.at[slot])

    def finished(c, s, h, value):
        tensor, q = s // subs, s % subs
        value = value.astype(f32)
        slot = (s * per + h) % WIDE
        copy = place(c, s, h)
        if not isinstance(c, int):
            pl.when((c * slots + s) * per + h >= WIDE)(copy.wait)
        elif (c * slots + s) * per + h >= WIDE:
            copy.wait()
        wide[slot] = value
        copy.start()
        square = value * value
        lanes = square[:, :LANES]
        for g in range(1, cw // LANES):
            lanes = lanes + square[:, g * LANES : (g + 1) * LANES]
        row = jnp.sum(lanes.T, axis=0, keepdims=True)
        if tensor == 0:
            at = pl.ds(c * per + hidden_side(q), 1)
            rows_d[at, :] = row if h == 0 else rows_d[at, :] + row
        else:
            at = ((tensor - 1) * subs + q) * per + h
            rows_gu[at : at + 1, :] = rows_gu[at : at + 1, :] + row

    def stage_a(p, h):
        part_copy(p, h).wait_recv()
        rows = half_rows(h)
        part[p, rows] = (ring[lax.rem(p, RING), rows] + from_out[p, rows].astype(f32)).astype(bf16)
        exchange_copy(p, h).start()

    def stage_b(c, s, h):
        p = c * slots + s
        rows = half_rows(h)
        exchange_copy(p, h).wait_recv()
        value = (part[p, rows].astype(f32) + from_in[p, rows].astype(f32)).astype(bf16)
        tot[p, rows] = value
        total_copy(p, h).start()
        finished(c, s, h, value)

    def stage_out(c, s, h):
        p = c * slots + s
        exchange_copy(p, h).wait_recv()
        finished(c, s, h, from_in[p, half_rows(h)])

    def behind(c, s, h, lag):
        steps = slots * per
        at = s * per + h - lag
        back = (-at + steps - 1) // steps if at < 0 else 0
        at += back * steps
        return c - back, at // per, at % per, back

    def guarded(c, lowest, fn):
        if isinstance(c, int):
            if c >= lowest:
                fn()
        elif lowest <= 1:
            fn()
        else:
            pl.when(c >= lowest)(fn)

    def work(c, s):
        tensor, q = s // subs, s % subs
        p = c * slots + s

        def middle(h):
            ca, sa, ha, ka = behind(c, s, h, A_LAG)
            guarded(c, ka, functools.partial(stage_a, ca * slots + sa, ha))
            cb, sb, hb, kb = behind(c, s, h, B_LAG)
            guarded(c, kb, functools.partial(stage_b, cb, sb, hb))

        if not isinstance(c, int) or c > 0 or s > 0:
            pl.when(is_mid)(lambda: middle(0))
        gathered(c, tensor, q)
        if tensor == 0:
            rows = pl.ds(pl.multiple_of(hidden_side(q) * LANES, LANES), LANES)
            value = jnp.dot(h_all[c, rows, :], og_ref[...], preferred_element_type=f32)
            value = jnp.concatenate([value[:, n * cw : (n + 1) * cw] for n in range(subs)], axis=0)
        elif tensor == 1:
            value = jnp.dot(xt[q], g_all[c], preferred_element_type=f32)
        else:
            value = jnp.dot(xt[q], u_all[c], preferred_element_type=f32)

        @pl.when(is_end)
        def _():
            for h in range(per):
                part[p, half_rows(h)] = value[half_rows(h)].astype(bf16)
                part_copy(p, h).start()
            for h in range(per):
                co, so, ho, ko = behind(c, s, h, OUT_LAG)
                guarded(c, ko, functools.partial(stage_out, co, so, ho))

        @pl.when(is_mid)
        def _():
            ring[lax.rem(p, RING)] = value
            middle(1)

    def input_term(c):
        cols = chunk_cols(c)
        term = contract(g_all[c], wg_ref[:, cols], 1, 1) + contract(u_all[c], wu_ref[:, cols], 1, 1)
        if isinstance(c, int) and c == 0:
            acc[...] = term
        else:
            acc[...] += term

    actions = {
        "forward": forward,
        "reduce": reduce_start,
        "combine": combine,
        "hidden": lambda c, tensor: hidden_step(c),
        "grads": lambda c, tensor: grads_step(c),
        "gather": gather_start,
    }

    def run(step, c):
        name, ahead, tensor = step
        target = c + ahead
        if isinstance(c, int):
            if target < chunks:
                actions[name](target, tensor)
        elif ahead == 0:
            actions[name](target, tensor)
        else:
            pl.when(target < chunks)(lambda: actions[name](target, tensor))

    m = 2 * (n_fs - 1)
    half = tok // 2
    ig_copy = remote(
        ig_send.at[pl.ds(pl.multiple_of((1 - t) * half, half), half)], ig_recv,
        misc.at[m], misc.at[m + 1], {"tp": 1 - t},
    )
    tap_peers = [
        remote(tap_all.at[f], tap_all.at[f], misc.at[2 * k], misc.at[2 * k + 1], {"fs": peers[k]})
        for k in range(n_fs - 1)
    ]
    tap_part = remote(tap_two, tap_out, misc.at[m + 2], misc.at[m + 3], {"rep": toward})
    tap_exchange = remote(tap_two, tap_in, misc.at[m + 2], misc.at[m + 4], {"rep": toward})
    tap_total = remote(tap_sum, tap_in, misc.at[m + 5], misc.at[m + 4], {"rep": outward})
    fs_rows = [
        remote(rows_d, rows_fs.at[k], misc.at[m + 8 + 2 * k], misc.at[m + 9 + 2 * k], {"fs": peers[k]})
        for k in range(n_fs - 1)
    ]
    tp_rows = remote(rows_gu, rows_tp, misc.at[m + 6], misc.at[m + 7], {"tp": 1 - t})

    outputs = [
        pltpu.make_async_copy(src, dst, out_sem.at[n])
        for n, (src, dst) in enumerate((
            (in_grad_ref, in_grad_out), (taps_out_ref, taps_out),
            (rows_down_ref, rows_down_out), (rows_gu_ref, rows_gu_out),
        ))
    ]

    def tap_first():
        for copy in tap_peers:
            copy.wait()
        for i in range(per):
            tap_two[i] = tap_all[i] + tap_all[i + 2]
        pl.when(is_end)(tap_part.start)

    def tap_second():
        tap_part.wait_recv()
        tap_two[...] = tap_two[...] + tap_out[...]
        tap_exchange.start()

    def tap_place():
        for c in range(chunks):
            for i in range(per):
                lane = (c * per + i) * LANES
                taps_out_ref[:, lane : lane + LANES] = tap_sum[i, c * KW : (c + 1) * KW, :]
        outputs[1].start()

    def input_start():
        ig_send[...] = acc[...].astype(bf16)
        ig_copy.start()

    def input_finish():
        ig_copy.wait()
        in_grad_ref[...] = (
            ig_send[pl.ds(pl.multiple_of(t * half, half), half), :].astype(f32) + ig_recv[...].astype(f32)
        ).astype(bf16)
        outputs[0].start()

    def body(c, last=False):
        for s in range(slots):
            for step in (FIRST_STEPS if isinstance(c, int) and c == 0 else STEPS)[s]:
                run(step, c)
            if last and s == 1:
                for copy in tap_peers:
                    copy.start()
            if last and s == 3:
                tap_first()
            if last and s == slots - 2:
                pl.when(is_mid)(tap_second)
            work(c, s)
        input_term(c)

    loads[0].wait()
    loads[1].wait()
    product(0, 0)
    pl.semaphore_wait(barrier, n_fs + 1 + jnp.where(is_mid, 1, 0))
    pl.when(t == 1)(lambda: pl.semaphore_wait(go_sem, 1))
    reduce_send(0, 0, range(2))
    loads[2].wait()
    product(0, 1)
    reduce_send(0, 1, range(2))
    reduce_send(0, 0, range(2, 4))
    reduce_send(0, 1, range(2, 4))
    loads[3].wait()
    loads[4].wait()
    reduce_start(0, 2)
    for q in range(subs):
        xt[q] = x_ref[:, q * cw : (q + 1) * cw].astype(f32).T.astype(bf16)
    rows_gu[...] = jnp.zeros_like(rows_gu)
    for copy in loads[5:]:
        copy.wait()
    combine(0, 0)

    @pl.when(t == 0)
    def _():
        pl.semaphore_signal(go_sem, inc=1, device_id={"tp": 1 - t}, device_id_type=MESH_ID)

    combine(0, 1)
    product(1, 0)
    combine(0, 2)
    hidden_step(0)
    grads_step(0)
    gather_start(0, 1)
    reduce_send(1, 0)
    reduce_start(1, 1)
    body(0)

    @pl.loop(1, chunks - 1)
    def _(c):
        body(c)

    body(chunks - 1, last=True)
    input_start()
    down_last = total_pieces - slots + subs - 1

    steps = total_pieces * per

    @pl.when(is_end)
    def _():
        for k in range(steps - OUT_LAG, steps):
            p = k // per
            if k == steps - 1:
                input_finish()
                tap_exchange.wait_recv()
                tap_sum[...] = tap_in[...]
                tap_place()
            stage_out(p // slots, p % slots, k % per)
            if k == max(steps - OUT_LAG, (down_last + 1) * per - 1):
                for copy in fs_rows:
                    copy.start()

    @pl.when(is_mid)
    def _():
        for copy in fs_rows:
            copy.start()
        for k in range(steps, steps + B_LAG):
            if k - A_LAG < steps:
                stage_a((k - A_LAG) // per, (k - A_LAG) % per)
            p = (k - B_LAG) // per
            stage_b(p // slots, p % slots, (k - B_LAG) % per)
            if k == steps:
                tap_exchange.wait_recv()
                tap_sum[...] = tap_two[...] + tap_in[...]
                tap_total.start()
                input_finish()
                tap_place()

    tp_rows.start()

    def all_sent(ref, sem):
        remote(ref, ref, sem, sem, {"tp": 1 - t}).wait_send()

    for n in range(6):
        rows = halves[n % 2]
        all_sent(recv_part.at[:, :, n, 0 : rows.stop - rows.start], rs_send.at[n])
    blocks = chunks * 3
    for slot in range(2):
        all_sent(part.at[0:blocks, 0 : own_rows // 2], ag_send.at[slot])
    for slot in range(2, 4):
        all_sent(part.at[0 : blocks - 2, 0 : own_rows // 4], ag_send.at[slot])
    all_sent(part.at[0:2, 0 : own_rows // 2], ag_send.at[4])
    all_sent(part, a_send.at[0])
    tap_part.wait_send()

    @pl.when(is_mid)
    def _():
        all_sent(tot, b_send.at[0])

    for k in range(steps - WIDE, steps):
        p = k // per
        place(p // slots, p % slots, k % per).wait()
    for copy in fs_rows:
        copy.wait()
    rows_down_ref[...] = rows_d[...] + (rows_fs[0] + rows_fs[1] + rows_fs[2])
    outputs[2].start()
    tp_rows.wait()
    rows_gu_ref[...] = rows_gu[...] + rows_tp[...]
    outputs[3].start()
    for copy in outputs:
        copy.wait()

    @pl.when(is_mid)
    def _():
        tap_total.wait_send()


def finish_kernel(
    gate, up, down, in_grad, taps, rows_gu, rows_d,
    gate_out, up_out, down_out, in_grad_out, taps_out, rows_gate_out, rows_up_out, rows_down_out,
    rows_gate, rows_up, rows_down, sems,
):
    copies = []

    def send(src, dst):
        copy = pltpu.make_async_copy(src, dst, sems.at[len(copies)])
        copy.start()
        copies.append(copy)

    for src, dst in ((gate, gate_out), (up, up_out), (down, down_out), (in_grad, in_grad_out), (taps, taps_out)):
        send(src, dst)
    groups = rows_gate.shape[0] // LANES
    for i in range(groups):
        rows_gate[pl.ds(i * LANES, LANES)] = rows_gu[i]
        rows_up[pl.ds(i * LANES, LANES)] = rows_gu[groups + i]
    for i in range(rows_down.shape[0] // LANES):
        rows_down[pl.ds(i * LANES, LANES)] = rows_d[i]
    for src, dst in ((rows_gate, rows_gate_out), (rows_up, rows_up_out), (rows_down, rows_down_out)):
        send(src, dst)
    for copy in copies:
        copy.wait()


def fits(shape, inputs, w_gate):
    n_rep, n_fs, n_tp = shape["rep"], shape["fs"], shape["tp"]
    tok, feat = inputs.shape
    return (
        n_rep == 4 and n_fs == 4 and n_tp == 2 and feat == 2 * CW and 3 * CW <= w_gate.shape[1]
        and w_gate.shape[1] % CW == 0 and w_gate.shape[1] <= 1536 and tok % (2 * LANES) == 0 and tok <= 512
    )


def fused_shards(shape, inputs, w_gate, w_up, conv_taps, w_down, out_grad):
    if not fits(shape, inputs, w_gate):
        return shards(inputs, w_gate, w_up, conv_taps, w_down, out_grad)
    n_rep, n_fs = shape["rep"], shape["fs"]
    tok, feat = inputs.shape
    hid = w_gate.shape[1]
    cw = CW
    chunks = hid // cw
    subs = feat // cw
    per = cw // LANES
    pieces = chunks * 3 * subs
    span = tok // 2 + HALO
    cut = -(-span // (2 * HALO)) * HALO
    bf16, f32 = jnp.bfloat16, jnp.float32
    vmem = pl.BlockSpec(memory_space=pltpu.VMEM)
    hbm = pl.BlockSpec(memory_space=pltpu.HBM)
    anywhere = pl.BlockSpec(memory_space=pl.ANY)
    dma = pltpu.SemaphoreType.DMA
    local = pltpu.VMEM
    whole = jax.ShapeDtypeStruct
    in_grad, down, gate, up, taps, rows_gu, rows_d = pl.pallas_call(
        functools.partial(layer_kernel, n_rep, n_fs),
        out_shape=(
            local((tok // 2, feat), bf16),
            local((hid, feat), f32),
            local((feat, hid), f32),
            local((feat, hid), f32),
            local((KW, hid), f32),
            local((2 * subs * per, LANES), f32),
            local((chunks * per, LANES), f32),
        ),
        in_specs=[hbm] * 6,
        out_specs=(anywhere,) * 7,
        scratch_shapes=[
            local((tok, feat), bf16),
            local((feat, hid), bf16),
            local((feat, hid), bf16),
            local((KW, hid), bf16),
            local((hid, feat), bf16),
            local((tok, feat), bf16),
            local((subs, cw, tok), bf16),
            local((chunks, 3, n_fs, span, LANES), bf16),
            local((chunks, 3, 6, cut, LANES), bf16),
            local((chunks, 3, 2, cut, LANES), bf16),
            local((4, span, LANES), f32),
            local((chunks, cw, tok), bf16),
            local((chunks, tok, cw), bf16),
            local((chunks, tok, cw), bf16),
            local((RING, cw, cw), f32),
            local((WIDE, LANES, cw), f32),
            local((pieces, cw, cw), bf16),
            local((pieces, cw, cw), bf16),
            local((pieces, cw, cw), bf16),
            local((pieces, cw, cw), bf16),
            local((tok, feat), f32),
            local((tok, feat), bf16),
            local((tok // 2, feat), bf16),
            local((tok // 2, feat), bf16),
            local((KW, hid), f32),
            local((2 * subs * per, LANES), f32),
            local((chunks * per, LANES), f32),
            local((n_fs, chunks * KW, LANES), f32),
            local((per, chunks * KW, LANES), f32),
            local((per, chunks * KW, LANES), f32),
            local((per, chunks * KW, LANES), f32),
            local((per, chunks * KW, LANES), f32),
            local((2 * subs * per, LANES), f32),
            local((chunks * per, LANES), f32),
            local((2 * subs * per, LANES), f32),
            local((n_fs - 1, chunks * per, LANES), f32),
            dma((6,)), dma((36,)), dma((5,)), dma((24,)),
            dma((1,)), dma((KEEP,)), dma((KEEP,)), dma((1,)), dma((WIDE,)), dma((4,)), dma((9,)), pltpu.SemaphoreType.REGULAR,
            dma((4 * (n_fs - 1) + 8,)),
        ],
        compiler_params=pltpu.CompilerParams(
            collective_id=0, has_side_effects=True, vmem_limit_bytes=50 * 1024 * 1024
        ),
    )(inputs, w_gate, w_up, conv_taps, w_down, out_grad)
    gate, up, down, in_grad, taps, rows_gate, rows_up, rows_down = pl.pallas_call(
        finish_kernel,
        out_shape=(
            whole((feat, hid), f32), whole((feat, hid), f32), whole((hid, feat), f32),
            whole((tok // 2, feat), bf16), whole((KW, hid), f32),
            whole((feat,), f32), whole((feat,), f32), whole((hid,), f32),
        ),
        in_specs=[anywhere] * 5 + [vmem] * 2,
        out_specs=(anywhere,) * 8,
        scratch_shapes=[local((feat,), f32), local((feat,), f32), local((hid,), f32), dma((8,))],
        compiler_params=pltpu.CompilerParams(vmem_limit_bytes=24 * 1024 * 1024),
    )(gate, up, down, in_grad, taps, rows_gu, rows_d)
    return (in_grad, gate, up, down, taps, rows_gate, rows_up, rows_down)


def solution(mesh):
    return jax.shard_map(
        functools.partial(fused_shards, dict(mesh.shape)),
        mesh=mesh,
        in_specs=(
            P("rep", "fs"),
            P("fs", "tp"),
            P("fs", "tp"),
            P(None, "tp"),
            P("tp", "fs"),
            P("rep", "fs"),
        ),
        out_specs=(
            P(("rep", "tp"), "fs"),
            P("fs", "tp"),
            P("fs", "tp"),
            P("tp", "fs"),
            P(None, "tp"),
            P("fs"),
            P("fs"),
            P("tp"),
        ),
        check_vma=False,
    )
```

```python
import functools

import jax
import jax.numpy as jnp
from jax import lax
from jax.experimental import pallas as pl
from jax.experimental.pallas import tpu as pltpu
from jax.sharding import PartitionSpec as P

KW = 3


def shift_down(values, lag_rows):
    if lag_rows == 0:
        return values
    padding = jnp.zeros_like(values[:lag_rows])
    return jnp.concatenate([padding, values[:-lag_rows]], axis=0)


def shift_up(values, lag_rows):
    if lag_rows == 0:
        return values
    padding = jnp.zeros_like(values[:lag_rows])
    return jnp.concatenate([values[lag_rows:], padding], axis=0)


def contract(left, right, left_dim, right_dim):
    return lax.dot_general(
        left, right, (((left_dim,), (right_dim,)), ((), ())), preferred_element_type=jnp.float32
    )


def row_norms(grad_gate, grad_up, grad_down):
    gate_rows = jnp.sum(grad_gate * grad_gate, axis=1)
    up_rows = jnp.sum(grad_up * grad_up, axis=1)
    down_rows = jnp.sum(grad_down * grad_down, axis=1)
    gate_rows, up_rows = lax.psum((gate_rows, up_rows), "tp")
    down_rows = lax.psum(down_rows, "fs")
    return (gate_rows, up_rows, down_rows)


def shards(inputs, w_gate, w_up, conv_taps, w_down, out_grad):
    tap_weights = conv_taps.astype(jnp.float32)
    gate_part = jnp.dot(inputs, w_gate, preferred_element_type=jnp.float32)
    up_part = jnp.dot(inputs, w_up, preferred_element_type=jnp.float32)
    act_part = contract(out_grad, w_down, 1, 1)
    gate_sum, up_sum, act_sum = (
        lax.psum(gate_part.astype(jnp.bfloat16), "fs").astype(jnp.float32),
        lax.psum(up_part.astype(jnp.bfloat16), "fs").astype(jnp.float32),
        lax.psum(act_part.astype(jnp.bfloat16), "fs").astype(jnp.float32),
    )
    gate_pre = gate_sum.astype(jnp.bfloat16)
    up_val = up_sum.astype(jnp.bfloat16)
    act_grad = act_sum.astype(jnp.bfloat16)
    gate_float = gate_pre.astype(jnp.float32)
    up_float = up_val.astype(jnp.float32)
    act_float = act_grad.astype(jnp.float32)
    shifted = [shift_down(gate_float, KW - 1 - tap_index) for tap_index in range(KW)]
    pre_act = tap_weights[0] * shifted[0]
    for tap_index in range(1, KW):
        pre_act = pre_act + tap_weights[tap_index] * shifted[tap_index]
    sigmoid_pre = jax.nn.sigmoid(pre_act)
    hidden = (pre_act * sigmoid_pre * up_float).astype(jnp.bfloat16)
    up_grad = (act_float * pre_act * sigmoid_pre).astype(jnp.bfloat16)
    pre_grad = act_float * up_float * sigmoid_pre * (1.0 + pre_act * (1.0 - sigmoid_pre))
    gate_acc = tap_weights[0] * shift_up(pre_grad, KW - 1)
    for tap_index in range(1, KW):
        gate_acc = gate_acc + tap_weights[tap_index] * shift_up(pre_grad, KW - 1 - tap_index)
    gate_grad = gate_acc.astype(jnp.bfloat16)
    gate_rows = gate_grad
    up_rows = up_grad
    in_grad = lax.psum_scatter(
        (contract(gate_rows, w_gate, 1, 1) + contract(up_rows, w_up, 1, 1)).astype(jnp.bfloat16),
        "tp",
        scatter_dimension=0,
        tiled=True,
    )
    grad_gate = contract(inputs, gate_grad, 0, 0)
    grad_up = contract(inputs, up_grad, 0, 0)
    grad_down = contract(hidden, out_grad, 0, 0)
    grad_taps = jnp.stack(
        [jnp.sum(shifted[tap_index] * pre_grad, axis=0) for tap_index in range(KW)]
    )
    grad_gate, grad_up, grad_down, grad_taps = (
        lax.psum(grad_gate.astype(jnp.bfloat16), "rep").astype(jnp.float32),
        lax.psum(grad_up.astype(jnp.bfloat16), "rep").astype(jnp.float32),
        lax.psum(grad_down.astype(jnp.bfloat16), "rep").astype(jnp.float32),
        lax.psum(grad_taps.astype(jnp.bfloat16), "rep").astype(jnp.float32),
    )
    gate_rows, up_rows, down_rows = row_norms(grad_gate, grad_up, grad_down)
    weight_grads = (grad_gate, grad_up, grad_down, grad_taps, gate_rows, up_rows, down_rows)
    grad_gate, grad_up, grad_down, grad_taps, gate_rows, up_rows, down_rows = weight_grads
    return (in_grad, grad_gate, grad_up, grad_down, grad_taps, gate_rows, up_rows, down_rows)


LANES = 128
CW = 256
HALO = 16
A_LAG = 1
B_LAG = 4
OUT_LAG = 18
RING = 2
WIDE = 4
KEEP = 24
MESH_ID = pl.DeviceIdType.MESH

STEPS = (
    (("grads", 0, 0), ("gather", 0, 1), ("reduce", 1, 0)),
    (("forward", 0, 1), ("gather", 0, 2)),
    (("combine", 1, 0), ("combine", 1, 1), ("reduce", 1, 2)),
    (("forward", 0, 2),),
    (("hidden", 1, 0), ("combine", 1, 2), ("reduce", 2, 1)),
    (("forward", 1, 0),),
)
FIRST_STEPS = ((), (("gather", 0, 2),), (), STEPS[2] + STEPS[3]) + STEPS[4:]


def layer_kernel(
    n_rep, n_fs,
    x_hbm, wg_hbm, wu_hbm, taps_hbm, wd_hbm, og_hbm,
    in_grad_out, down_ref, gate_ref, up_ref, taps_out, rows_gu_out, rows_down_out,
    x_ref, wg_ref, wu_ref, taps_ref, wd_ref, og_ref,
    xt, send_part, recv_part, pair_part, held, h_all, g_all, u_all, ring, wide, part, from_out, from_in, tot,
    acc, ig_send, ig_recv, in_grad_ref, taps_out_ref, rows_gu_ref, rows_down_ref, tap_all, tap_two, tap_out, tap_in, tap_sum, rows_gu, rows_d, rows_tp, rows_fs,
    rs_send, rs_recv, ag_send, ag_recv, a_send, out_recv, in_recv, b_send, wide_sem, out_sem, loc_sem, go_sem, misc,
):
    tok, feat = x_ref.shape
    cw = CW
    chunks = wg_ref.shape[1] // cw
    subs = feat // cw
    own_rows = tok // 2
    span = own_rows + HALO
    slots = 3 * subs
    total_pieces = chunks * slots
    per = cw // LANES
    f32, bf16 = jnp.float32, jnp.bfloat16
    r = lax.axis_index("rep")
    f = lax.axis_index("fs")
    t = lax.axis_index("tp")
    half_rep = n_rep // 2
    is_left = r < half_rep
    toward = jnp.where(is_left, r + 1, r - 1)
    outward = jnp.where(is_left, r - 1, r + 1)
    is_end = jnp.logical_or(r == 0, r == n_rep - 1)
    is_mid = jnp.logical_not(is_end)
    beside = f + 1 - 2 * lax.rem(f, 2)
    across = lax.rem(f + 2, 4)
    corner = lax.rem(beside + 2, 4)
    peers = [beside, across, corner]
    side = lax.rem(f, 2)
    top = f // 2
    own_cols = pl.ds(pl.multiple_of(side * LANES, LANES), LANES)
    own_toks = pl.ds(pl.multiple_of(top * own_rows, own_rows), own_rows)

    barrier = pltpu.get_barrier_semaphore()
    for k in range(n_fs - 1):
        pl.semaphore_signal(barrier, inc=1, device_id={"fs": peers[k]}, device_id_type=MESH_ID)
    pl.semaphore_signal(barrier, inc=1, device_id={"tp": 1 - t}, device_id_type=MESH_ID)
    pl.semaphore_signal(barrier, inc=1, device_id={"rep": toward}, device_id_type=MESH_ID)

    @pl.when(is_mid)
    def _():
        pl.semaphore_signal(barrier, inc=1, device_id={"rep": outward}, device_id_type=MESH_ID)

    loads = []

    def load(src, dst):
        copy = pltpu.make_async_copy(src, dst, loc_sem.at[len(loads)])
        copy.start()
        loads.append(copy)

    first = slice(0, cw)
    load(x_hbm, x_ref)
    load(wg_hbm.at[:, first], wg_ref.at[:, first])
    load(wu_hbm.at[:, first], wu_ref.at[:, first])
    load(og_hbm, og_ref)
    load(wd_hbm.at[first], wd_ref.at[first])
    load(taps_hbm, taps_ref)
    if chunks > 1:
        rest = slice(cw, chunks * cw)
        load(wg_hbm.at[:, rest], wg_ref.at[:, rest])
        load(wu_hbm.at[:, rest], wu_ref.at[:, rest])
        load(wd_hbm.at[rest], wd_ref.at[rest])

    def remote(src, dst, send, recv, device):
        return pltpu.make_async_remote_copy(
            src_ref=src, dst_ref=dst, send_sem=send, recv_sem=recv,
            device_id=device, device_id_type=MESH_ID,
        )

    def chunk_cols(c):
        if isinstance(c, int):
            return slice(c * cw, (c + 1) * cw)
        return pl.ds(pl.multiple_of(c * cw, cw), cw)

    cut = recv_part.shape[3]
    halves = (slice(0, cut), slice(cut, span))

    def rs_copy(c, tensor, n):
        s = (lax.rem(c, 2) * 3 + tensor) * 6 + n
        side_of = n % 2
        near, far = (beside, across) if side_of == 0 else (across, beside)
        rows = halves[side_of]
        size = rows.stop - rows.start
        owner = corner if n < 2 else near
        target = near if n < 4 else far
        if n < 4:
            src = send_part.at[c, tensor, owner, rows]
        else:
            src = pair_part.at[c, tensor, side_of, 0:size]
        return remote(
            src, recv_part.at[c, tensor, n, 0:size], rs_send.at[n], rs_recv.at[s], {"fs": target}
        )

    def product(c, tensor):
        cols = chunk_cols(c)
        if tensor == 0:
            value = jnp.dot(x_ref[...], wg_ref[:, cols], preferred_element_type=f32)
        elif tensor == 1:
            value = jnp.dot(x_ref[...], wu_ref[:, cols], preferred_element_type=f32)
        else:
            value = contract(og_ref[...], wd_ref[cols, :], 1, 1)
        value = value.astype(bf16)
        for g in range(n_fs):
            row = (g // 2) * (own_rows - HALO)
            lane = (g % 2) * LANES
            send_part[c, tensor, g] = value[row : row + span, lane : lane + LANES]

    def reduce_send(c, tensor, steps=range(4)):
        for n in steps:
            rs_copy(c, tensor, n).start()

    def reduce_start(c, tensor):
        product(c, tensor)
        reduce_send(c, tensor)

    def combine(c, tensor):
        for n in range(2):
            rows = halves[n]
            size = rows.stop - rows.start
            rs_copy(c, tensor, n).wait_recv()
            mine = send_part[c, tensor, across if n == 0 else beside, rows]
            pair_part[c, tensor, n, 0:size] = (
                mine.astype(f32) + recv_part[c, tensor, n, 0:size].astype(f32)
            ).astype(bf16)
            rs_copy(c, tensor, 4 + n).start()

    def reduced(c, tensor):
        parts = []
        for n in range(2):
            rows = halves[n]
            size = rows.stop - rows.start
            rs_copy(c, tensor, 2 + n).wait_recv()
            value = send_part[c, tensor, f, rows].astype(f32) + recv_part[c, tensor, 2 + n, 0:size].astype(f32)
            rs_copy(c, tensor, 4 + n).wait_recv()
            parts.append(value + recv_part[c, tensor, 4 + n, 0:size].astype(f32))
        return jnp.concatenate(parts, axis=0).astype(bf16).astype(f32)

    def block(c, tensor, owner, part_of=None):
        col = lax.rem(owner, 2) * LANES
        row = (owner // 2) * own_rows
        if tensor == 0:
            size = LANES if part_of is None else LANES // 2
            start = col + (0 if part_of is None else part_of * size)
            return h_all.at[
                c, pl.ds(pl.multiple_of(start, size), size), pl.ds(pl.multiple_of(row, own_rows), own_rows)
            ]
        size = own_rows if part_of is None else own_rows // 2
        start = row + (0 if part_of is None else part_of * size)
        ref = g_all if tensor == 1 else u_all
        return ref.at[c, pl.ds(pl.multiple_of(start, size), size), pl.ds(pl.multiple_of(col, LANES), LANES)]

    def ag_copy(c, tensor, step, owner):
        s = (lax.rem(c, 2) * 3 + tensor) * 4
        if step == 0:
            ref, slot, target = block(c, tensor, owner), 0, beside
        elif step == 1:
            ref, slot, target = block(c, tensor, owner), 1, across
        elif step == 2:
            ref, slot, target = block(c, tensor, owner, 1), 2, beside
        else:
            ref, slot, target = block(c, tensor, owner, 0), 3, across
        return remote(ref, ref, ag_send.at[slot], ag_recv.at[s + slot], {"fs": target})

    def direct(c, tensor):
        return isinstance(c, int) and c == 0 and tensor < 2

    def corner_copy(c, tensor, owner):
        ref = block(c, tensor, owner)
        return remote(ref, ref, ag_send.at[4], ag_recv.at[tensor * 4 + 2], {"fs": corner})

    def gather_start(c, tensor):
        for step in (0, 1):
            ag_copy(c, tensor, step, f).start()
        if direct(c, tensor):
            corner_copy(c, tensor, f).start()

    def forward(c, tensor):
        ag_copy(c, tensor, 0, beside).wait_recv()
        ag_copy(c, tensor, 3, beside).start()
        ag_copy(c, tensor, 1, across).wait_recv()
        ag_copy(c, tensor, 2, across).start()

    def gathered(c, tensor, q):
        if direct(c, tensor):
            if q == 0:
                ag_copy(c, tensor, 1, across).wait_recv()
            if q == tensor ^ 1:
                ag_copy(c, tensor, 0, beside).wait_recv()
                corner_copy(c, tensor, corner).wait_recv()
        elif q == (1 if tensor == 0 else 0):
            ag_copy(c, tensor, 2, corner).wait_recv()
            ag_copy(c, tensor, 3, corner).wait_recv()

    def hidden_side(q):
        return side if q == 0 else 1 - side

    def own(value):
        return jnp.where(top == 0, value[:own_rows], value[HALO:])

    row_ids = lax.broadcasted_iota(jnp.int32, (span, LANES), 0)

    def down(value, lag):
        if lag == 0:
            return value
        return jnp.where(row_ids >= lag, pltpu.roll(value, lag, 0), 0.0)

    def up(value, lag):
        if lag == 0:
            return value
        return jnp.where(row_ids < span - lag, pltpu.roll(value, span - lag, 0), 0.0)

    def own_weights(c):
        cols = pl.ds(pl.multiple_of(c * cw + side * LANES, LANES), LANES)
        return taps_ref[:, cols].astype(f32)

    def hidden_step(c):
        weights = own_weights(c)
        gate = reduced(c, 0)
        pre = weights[0:1] * down(gate, KW - 1)
        for j in range(1, KW):
            pre = pre + weights[j : j + 1] * down(gate, KW - 1 - j)
        sig = 1.0 / (1.0 + jnp.exp(-pre))
        up_val = reduced(c, 1)
        h_all[c, own_cols, own_toks] = own(pre * sig * up_val).T.astype(bf16)
        gather_start(c, 0)
        held[0] = gate
        held[1] = up_val
        held[2] = pre
        held[3] = sig

    def grads_step(c):
        weights = own_weights(c)
        gate, up_val, pre, sig = held[0], held[1], held[2], held[3]
        act = reduced(c, 2)
        pre_grad = act * up_val * sig * (1.0 + pre * (1.0 - sig))
        grad = weights[0:1] * up(pre_grad, KW - 1)
        for j in range(1, KW):
            grad = grad + weights[j : j + 1] * up(pre_grad, KW - 1 - j)
        g_all[c, own_toks, own_cols] = own(grad).astype(bf16)
        u_all[c, own_toks, own_cols] = own(act * (pre * sig)).astype(bf16)
        for j in range(KW):
            tap_all[f, pl.ds(c * KW + j, 1), :] = jnp.sum(
                own(down(gate, KW - 1 - j) * pre_grad), axis=0, keepdims=True
            )

    def half_rows(h):
        return slice(h * LANES, (h + 1) * LANES)

    def part_copy(p, h):
        rows = half_rows(h)
        s = lax.rem(p * per + h, KEEP)
        return remote(part.at[p, rows], from_out.at[p, rows], a_send.at[0], out_recv.at[s], {"rep": toward})

    def exchange_copy(p, h):
        rows = half_rows(h)
        s = lax.rem(p * per + h, KEEP)
        return remote(part.at[p, rows], from_in.at[p, rows], a_send.at[0], in_recv.at[s], {"rep": toward})

    def total_copy(p, h):
        rows = half_rows(h)
        s = lax.rem(p * per + h, KEEP)
        return remote(tot.at[p, rows], from_in.at[p, rows], b_send.at[0], in_recv.at[s], {"rep": outward})

    def piece_rows(base, h):
        if isinstance(base, int) and isinstance(h, int):
            return slice(base + h * LANES, base + (h + 1) * LANES)
        return pl.ds(pl.multiple_of(base + h * LANES, LANES), LANES)

    def place(c, s, h):
        tensor, q = s // subs, s % subs
        slot = (s * per + h) % WIDE
        if tensor == 0:
            dst = down_ref.at[piece_rows(c * cw, hidden_side(q)), h * cw : (h + 1) * cw]
        elif tensor == 1:
            dst = gate_ref.at[piece_rows(q * cw, h), chunk_cols(c)]
        else:
            dst = up_ref.at[piece_rows(q * cw, h), chunk_cols(c)]
        return pltpu.make_async_copy(wide.at[slot], dst, wide_sem.at[slot])

    def finished(c, s, h, value):
        tensor, q = s // subs, s % subs
        value = value.astype(f32)
        slot = (s * per + h) % WIDE
        copy = place(c, s, h)
        if not isinstance(c, int):
            pl.when((c * slots + s) * per + h >= WIDE)(copy.wait)
        elif (c * slots + s) * per + h >= WIDE:
            copy.wait()
        wide[slot] = value
        copy.start()
        square = value * value
        lanes = square[:, :LANES]
        for g in range(1, cw // LANES):
            lanes = lanes + square[:, g * LANES : (g + 1) * LANES]
        row = jnp.sum(lanes.T, axis=0, keepdims=True)
        if tensor == 0:
            at = pl.ds(c * per + hidden_side(q), 1)
            rows_d[at, :] = row if h == 0 else rows_d[at, :] + row
        else:
            at = ((tensor - 1) * subs + q) * per + h
            rows_gu[at : at + 1, :] = rows_gu[at : at + 1, :] + row

    def stage_a(p, h):
        part_copy(p, h).wait_recv()
        rows = half_rows(h)
        part[p, rows] = (ring[lax.rem(p, RING), rows] + from_out[p, rows].astype(f32)).astype(bf16)
        exchange_copy(p, h).start()

    def stage_b(c, s, h):
        p = c * slots + s
        rows = half_rows(h)
        exchange_copy(p, h).wait_recv()
        value = (part[p, rows].astype(f32) + from_in[p, rows].astype(f32)).astype(bf16)
        tot[p, rows] = value
        total_copy(p, h).start()
        finished(c, s, h, value)

    def stage_out(c, s, h):
        p = c * slots + s
        exchange_copy(p, h).wait_recv()
        finished(c, s, h, from_in[p, half_rows(h)])

    def behind(c, s, h, lag):
        steps = slots * per
        at = s * per + h - lag
        back = (-at + steps - 1) // steps if at < 0 else 0
        at += back * steps
        return c - back, at // per, at % per, back

    def guarded(c, lowest, fn):
        if isinstance(c, int):
            if c >= lowest:
                fn()
        elif lowest <= 1:
            fn()
        else:
            pl.when(c >= lowest)(fn)

    def middle_steps(c, s, h):
        ca, sa, ha, ka = behind(c, s, h, A_LAG)
        guarded(c, ka, functools.partial(stage_a, ca * slots + sa, ha))
        cb, sb, hb, kb = behind(c, s, h, B_LAG)
        guarded(c, kb, functools.partial(stage_b, cb, sb, hb))

    def work(c, s):
        tensor, q = s // subs, s % subs
        p = c * slots + s

        middle = functools.partial(middle_steps, c, s)
        gathered(c, tensor, q)
        if tensor == 0:
            rows = pl.ds(pl.multiple_of(hidden_side(q) * LANES, LANES), LANES)
            value = jnp.dot(h_all[c, rows, :], og_ref[...], preferred_element_type=f32)
            value = jnp.concatenate([value[:, n * cw : (n + 1) * cw] for n in range(subs)], axis=0)
        elif tensor == 1:
            value = jnp.dot(xt[q], g_all[c], preferred_element_type=f32)
        else:
            value = jnp.dot(xt[q], u_all[c], preferred_element_type=f32)

        @pl.when(is_end)
        def _():
            for h in range(per):
                part[p, half_rows(h)] = value[half_rows(h)].astype(bf16)
                part_copy(p, h).start()
            for h in range(per):
                co, so, ho, ko = behind(c, s, h, OUT_LAG)
                guarded(c, ko, functools.partial(stage_out, co, so, ho))

        @pl.when(is_mid)
        def _():
            ring[lax.rem(p, RING)] = value
            middle(1)

    def input_term(c):
        cols = chunk_cols(c)
        term = contract(g_all[c], wg_ref[:, cols], 1, 1) + contract(u_all[c], wu_ref[:, cols], 1, 1)
        if isinstance(c, int) and c == 0:
            acc[...] = term
        else:
            acc[...] += term

    actions = {
        "forward": forward,
        "reduce": reduce_start,
        "combine": combine,
        "hidden": lambda c, tensor: hidden_step(c),
        "grads": lambda c, tensor: grads_step(c),
        "gather": gather_start,
    }

    def run(step, c):
        name, ahead, tensor = step
        target = c + ahead
        if isinstance(c, int):
            if target < chunks:
                actions[name](target, tensor)
        elif ahead == 0:
            actions[name](target, tensor)
        else:
            pl.when(target < chunks)(lambda: actions[name](target, tensor))

    m = 2 * (n_fs - 1)
    half = tok // 2
    ig_copy = remote(
        ig_send.at[pl.ds(pl.multiple_of((1 - t) * half, half), half)], ig_recv,
        misc.at[m], misc.at[m + 1], {"tp": 1 - t},
    )
    tap_peers = [
        remote(tap_all.at[f], tap_all.at[f], misc.at[2 * k], misc.at[2 * k + 1], {"fs": peers[k]})
        for k in range(n_fs - 1)
    ]
    tap_part = remote(tap_two, tap_out, misc.at[m + 2], misc.at[m + 3], {"rep": toward})
    tap_exchange = remote(tap_two, tap_in, misc.at[m + 2], misc.at[m + 4], {"rep": toward})
    tap_total = remote(tap_sum, tap_in, misc.at[m + 5], misc.at[m + 4], {"rep": outward})
    fs_rows = [
        remote(rows_d, rows_fs.at[k], misc.at[m + 8 + 2 * k], misc.at[m + 9 + 2 * k], {"fs": peers[k]})
        for k in range(n_fs - 1)
    ]
    tp_rows = remote(rows_gu, rows_tp, misc.at[m + 6], misc.at[m + 7], {"tp": 1 - t})

    outputs = [
        pltpu.make_async_copy(src, dst, out_sem.at[n])
        for n, (src, dst) in enumerate((
            (in_grad_ref, in_grad_out), (taps_out_ref, taps_out),
            (rows_down_ref, rows_down_out), (rows_gu_ref, rows_gu_out),
        ))
    ]

    def tap_first():
        for copy in tap_peers:
            copy.wait()
        for i in range(per):
            tap_two[i] = tap_all[i] + tap_all[i + 2]
        pl.when(is_end)(tap_part.start)

    def tap_second():
        tap_part.wait_recv()
        tap_two[...] = tap_two[...] + tap_out[...]
        tap_exchange.start()

    def tap_place():
        for c in range(chunks):
            for i in range(per):
                lane = (c * per + i) * LANES
                taps_out_ref[:, lane : lane + LANES] = tap_sum[i, c * KW : (c + 1) * KW, :]
        outputs[1].start()

    def input_start():
        ig_send[...] = acc[...].astype(bf16)
        ig_copy.start()

    def input_finish():
        ig_copy.wait()
        in_grad_ref[...] = (
            ig_send[pl.ds(pl.multiple_of(t * half, half), half), :].astype(f32) + ig_recv[...].astype(f32)
        ).astype(bf16)
        outputs[0].start()

    def body(c, last=False):
        for s in range(slots):
            if not isinstance(c, int) or c > 0 or s > 0:
                pl.when(is_mid)(functools.partial(middle_steps, c, s, 0))
            for step in (FIRST_STEPS if isinstance(c, int) and c == 0 else STEPS)[s]:
                run(step, c)
            if last and s == 1:
                for copy in tap_peers:
                    copy.start()
            if last and s == 3:
                tap_first()
            if last and s == slots - 2:
                pl.when(is_mid)(tap_second)
            work(c, s)
        input_term(c)

    loads[0].wait()
    loads[1].wait()
    product(0, 0)
    pl.semaphore_wait(barrier, n_fs + 1 + jnp.where(is_mid, 1, 0))
    pl.when(t == 1)(lambda: pl.semaphore_wait(go_sem, 1))
    reduce_send(0, 0, range(2))
    loads[2].wait()
    product(0, 1)
    reduce_send(0, 1, range(2))
    reduce_send(0, 0, range(2, 4))
    reduce_send(0, 1, range(2, 4))
    loads[3].wait()
    loads[4].wait()
    reduce_start(0, 2)
    for q in range(subs):
        xt[q] = x_ref[:, q * cw : (q + 1) * cw].astype(f32).T.astype(bf16)
    rows_gu[...] = jnp.zeros_like(rows_gu)
    for copy in loads[5:]:
        copy.wait()
    combine(0, 0)

    @pl.when(t == 0)
    def _():
        pl.semaphore_signal(go_sem, inc=1, device_id={"tp": 1 - t}, device_id_type=MESH_ID)

    combine(0, 1)
    product(1, 0)
    combine(0, 2)
    hidden_step(0)
    grads_step(0)
    gather_start(0, 1)
    reduce_send(1, 0)
    reduce_start(1, 1)
    body(0)

    @pl.loop(1, chunks - 1)
    def _(c):
        body(c)

    body(chunks - 1, last=True)
    input_start()
    down_last = total_pieces - slots + subs - 1

    steps = total_pieces * per

    @pl.when(is_end)
    def _():
        for k in range(steps - OUT_LAG, steps):
            p = k // per
            if k == steps - 1:
                input_finish()
                tap_exchange.wait_recv()
                tap_sum[...] = tap_in[...]
                tap_place()
            stage_out(p // slots, p % slots, k % per)
            if k == max(steps - OUT_LAG, (down_last + 1) * per - 1):
                for copy in fs_rows:
                    copy.start()

    @pl.when(is_mid)
    def _():
        for copy in fs_rows:
            copy.start()
        for k in range(steps, steps + B_LAG):
            if k - A_LAG < steps:
                stage_a((k - A_LAG) // per, (k - A_LAG) % per)
            p = (k - B_LAG) // per
            stage_b(p // slots, p % slots, (k - B_LAG) % per)
            if k == steps:
                tap_exchange.wait_recv()
                tap_sum[...] = tap_two[...] + tap_in[...]
                tap_total.start()
                input_finish()
                tap_place()

    tp_rows.start()

    def all_sent(ref, sem):
        remote(ref, ref, sem, sem, {"tp": 1 - t}).wait_send()

    for n in range(6):
        rows = halves[n % 2]
        all_sent(recv_part.at[:, :, n, 0 : rows.stop - rows.start], rs_send.at[n])
    blocks = chunks * 3
    for slot in range(2):
        all_sent(part.at[0:blocks, 0 : own_rows // 2], ag_send.at[slot])
    for slot in range(2, 4):
        all_sent(part.at[0 : blocks - 2, 0 : own_rows // 4], ag_send.at[slot])
    all_sent(part.at[0:2, 0 : own_rows // 2], ag_send.at[4])
    all_sent(part, a_send.at[0])
    tap_part.wait_send()

    @pl.when(is_mid)
    def _():
        all_sent(tot, b_send.at[0])

    for k in range(steps - WIDE, steps):
        p = k // per
        place(p // slots, p % slots, k % per).wait()
    for copy in fs_rows:
        copy.wait()
    rows_down_ref[...] = rows_d[...] + (rows_fs[0] + rows_fs[1] + rows_fs[2])
    outputs[2].start()
    tp_rows.wait()
    rows_gu_ref[...] = rows_gu[...] + rows_tp[...]
    outputs[3].start()
    for copy in outputs:
        copy.wait()

    @pl.when(is_mid)
    def _():
        tap_total.wait_send()


def finish_kernel(
    gate, up, down, in_grad, taps, rows_gu, rows_d,
    gate_out, up_out, down_out, in_grad_out, taps_out, rows_gate_out, rows_up_out, rows_down_out,
    rows_gate, rows_up, rows_down, sems,
):
    copies = []

    def send(src, dst):
        copy = pltpu.make_async_copy(src, dst, sems.at[len(copies)])
        copy.start()
        copies.append(copy)

    for src, dst in ((gate, gate_out), (up, up_out), (down, down_out), (in_grad, in_grad_out), (taps, taps_out)):
        send(src, dst)
    groups = rows_gate.shape[0] // LANES
    for i in range(groups):
        rows_gate[pl.ds(i * LANES, LANES)] = rows_gu[i]
        rows_up[pl.ds(i * LANES, LANES)] = rows_gu[groups + i]
    for i in range(rows_down.shape[0] // LANES):
        rows_down[pl.ds(i * LANES, LANES)] = rows_d[i]
    for src, dst in ((rows_gate, rows_gate_out), (rows_up, rows_up_out), (rows_down, rows_down_out)):
        send(src, dst)
    for copy in copies:
        copy.wait()


def fits(shape, inputs, w_gate):
    n_rep, n_fs, n_tp = shape["rep"], shape["fs"], shape["tp"]
    tok, feat = inputs.shape
    return (
        n_rep == 4 and n_fs == 4 and n_tp == 2 and feat == 2 * CW and 3 * CW <= w_gate.shape[1]
        and w_gate.shape[1] % CW == 0 and w_gate.shape[1] <= 1536 and tok % (2 * LANES) == 0 and tok <= 512
    )


def fused_shards(shape, inputs, w_gate, w_up, conv_taps, w_down, out_grad):
    if not fits(shape, inputs, w_gate):
        return shards(inputs, w_gate, w_up, conv_taps, w_down, out_grad)
    n_rep, n_fs = shape["rep"], shape["fs"]
    tok, feat = inputs.shape
    hid = w_gate.shape[1]
    cw = CW
    chunks = hid // cw
    subs = feat // cw
    per = cw // LANES
    pieces = chunks * 3 * subs
    span = tok // 2 + HALO
    cut = -(-span // (2 * HALO)) * HALO
    bf16, f32 = jnp.bfloat16, jnp.float32
    vmem = pl.BlockSpec(memory_space=pltpu.VMEM)
    hbm = pl.BlockSpec(memory_space=pltpu.HBM)
    anywhere = pl.BlockSpec(memory_space=pl.ANY)
    dma = pltpu.SemaphoreType.DMA
    local = pltpu.VMEM
    whole = jax.ShapeDtypeStruct
    in_grad, down, gate, up, taps, rows_gu, rows_d = pl.pallas_call(
        functools.partial(layer_kernel, n_rep, n_fs),
        out_shape=(
            local((tok // 2, feat), bf16),
            local((hid, feat), f32),
            local((feat, hid), f32),
            local((feat, hid), f32),
            local((KW, hid), f32),
            local((2 * subs * per, LANES), f32),
            local((chunks * per, LANES), f32),
        ),
        in_specs=[hbm] * 6,
        out_specs=(anywhere,) * 7,
        scratch_shapes=[
            local((tok, feat), bf16),
            local((feat, hid), bf16),
            local((feat, hid), bf16),
            local((KW, hid), bf16),
            local((hid, feat), bf16),
            local((tok, feat), bf16),
            local((subs, cw, tok), bf16),
            local((chunks, 3, n_fs, span, LANES), bf16),
            local((chunks, 3, 6, cut, LANES), bf16),
            local((chunks, 3, 2, cut, LANES), bf16),
            local((4, span, LANES), f32),
            local((chunks, cw, tok), bf16),
            local((chunks, tok, cw), bf16),
            local((chunks, tok, cw), bf16),
            local((RING, cw, cw), f32),
            local((WIDE, LANES, cw), f32),
            local((pieces, cw, cw), bf16),
            local((pieces, cw, cw), bf16),
            local((pieces, cw, cw), bf16),
            local((pieces, cw, cw), bf16),
            local((tok, feat), f32),
            local((tok, feat), bf16),
            local((tok // 2, feat), bf16),
            local((tok // 2, feat), bf16),
            local((KW, hid), f32),
            local((2 * subs * per, LANES), f32),
            local((chunks * per, LANES), f32),
            local((n_fs, chunks * KW, LANES), f32),
            local((per, chunks * KW, LANES), f32),
            local((per, chunks * KW, LANES), f32),
            local((per, chunks * KW, LANES), f32),
            local((per, chunks * KW, LANES), f32),
            local((2 * subs * per, LANES), f32),
            local((chunks * per, LANES), f32),
            local((2 * subs * per, LANES), f32),
            local((n_fs - 1, chunks * per, LANES), f32),
            dma((6,)), dma((36,)), dma((5,)), dma((24,)),
            dma((1,)), dma((KEEP,)), dma((KEEP,)), dma((1,)), dma((WIDE,)), dma((4,)), dma((9,)), pltpu.SemaphoreType.REGULAR,
            dma((4 * (n_fs - 1) + 8,)),
        ],
        compiler_params=pltpu.CompilerParams(
            collective_id=0, has_side_effects=True, vmem_limit_bytes=50 * 1024 * 1024
        ),
    )(inputs, w_gate, w_up, conv_taps, w_down, out_grad)
    gate, up, down, in_grad, taps, rows_gate, rows_up, rows_down = pl.pallas_call(
        finish_kernel,
        out_shape=(
            whole((feat, hid), f32), whole((feat, hid), f32), whole((hid, feat), f32),
            whole((tok // 2, feat), bf16), whole((KW, hid), f32),
            whole((feat,), f32), whole((feat,), f32), whole((hid,), f32),
        ),
        in_specs=[anywhere] * 5 + [vmem] * 2,
        out_specs=(anywhere,) * 8,
        scratch_shapes=[local((feat,), f32), local((feat,), f32), local((hid,), f32), dma((8,))],
        compiler_params=pltpu.CompilerParams(vmem_limit_bytes=24 * 1024 * 1024),
    )(gate, up, down, in_grad, taps, rows_gu, rows_d)
    return (in_grad, gate, up, down, taps, rows_gate, rows_up, rows_down)


def solution(mesh):
    return jax.shard_map(
        functools.partial(fused_shards, dict(mesh.shape)),
        mesh=mesh,
        in_specs=(
            P("rep", "fs"),
            P("fs", "tp"),
            P("fs", "tp"),
            P(None, "tp"),
            P("tp", "fs"),
            P("rep", "fs"),
        ),
        out_specs=(
            P(("rep", "tp"), "fs"),
            P("fs", "tp"),
            P("fs", "tp"),
            P("tp", "fs"),
            P(None, "tp"),
            P("fs"),
            P("fs"),
            P("tp"),
        ),
        check_vma=False,
    )
```
